32 devices in a mesh: grp: 2 (over y), tp: 4 (over z), dp: 4 (over x, core).
Axes of the slice: x: 2, y: 2, z: 4, core: 2. Of those that a mesh axis runs over, the one named last changes fastest.
Arguments:
- tokens: bfloat16 [128, 4096], P('grp', 'dp'), parts along dimension 0, may hold values from -6 to 6
- norm_gain: float32 [2, 4096], P(None, 'dp'), may hold values from 0.1 to 1.9
- w_query: bfloat16 [2, 4096, 512], P(None, 'dp', 'tp'), may hold values from -0.09375 to 0.09375
- w_key: bfloat16 [2, 4096, 512], P(None, 'dp', 'tp'), may hold values from -0.09375 to 0.09375
- w_value: bfloat16 [2, 4096, 512], P(None, 'dp', 'tp'), may hold values from -0.09375 to 0.09375
- w_outgate: bfloat16 [2, 4096, 512], P(None, 'dp', 'tp'), may hold values from -0.09375 to 0.09375
- gate_weight: bfloat16 [2, 4, 384, 2], P(None, 'tp'), may hold values from -0.3125 to 0.3125
- forget_bias: float32 [2, 4], P(None, 'tp'), may hold values from -2 to 4
- w_mix: bfloat16 [2, 512, 4096], P(None, 'tp', 'dp'), may hold values from -0.25 to 0.25
- memory: float32 [2, 128, 4, 128, 128], P(None, ('grp', 'dp'), 'tp'), parts along dimension 1, may hold values from -3 to 3
- normalizer: float32 [2, 128, 4, 128], P(None, ('grp', 'dp'), 'tp'), parts along dimension 1, may hold values from -3 to 3
- stabilizer: float32 [2, 128, 4], P(None, ('grp', 'dp'), 'tp'), parts along dimension 1, may hold values from -4 to 4
Outputs:
- result: bfloat16 [128, 4096], P('grp', 'dp'), parts along dimension 0
- new_memory: float32 [2, 128, 4, 128, 128], P(None, ('grp', 'dp'), 'tp'), parts along dimension 1
- new_normalizer: float32 [2, 128, 4, 128], P(None, ('grp', 'dp'), 'tp'), parts along dimension 1
- new_stabilizer: float32 [2, 128, 4], P(None, ('grp', 'dp'), 'tp'), parts along dimension 1
The draws below stay inside these ranges and needn't reach their ends.
There are 2 independent parts, one for each index of `grp`. The reference program is written for one: setup_inputs(seed, part) draws one part's arguments, and reference() takes and returns one part's arrays. A program takes and returns all parts, laid end to end along the dimension named above; an argument that names none is the same for every part. Nothing has to cross between parts.
All inputs are finite; a program needn't handle non-finite values.
Results may differ from the reference program's by a relative error of at most 0.018.
Values may be sent and summed in bfloat16 or wider, within the bound.
A program may use at most 64 MiB of HBM per device.

```python
import jax
import jax.numpy as jnp
from jax import lax

D = 4096
DK = 128
BLOCKS = 2
HEADS = 4
INNER = 512
SEQS = 64


def shard_levels(key, shape, cuts, least, top_value):
    factor_of, own = 1.0, jax.random.fold_in(key, 6)
    for axis_at, parts in cuts:
        steps = jnp.exp(jax.random.uniform(jax.random.fold_in(own, axis_at), (parts,), jnp.float32, least / len(cuts), top_value / len(cuts)))
        factor_of = factor_of * jnp.repeat(steps, shape[axis_at] // parts).reshape([-1 if axis == axis_at else 1 for axis in range(len(shape))])
    return factor_of


def gaussian(stream_key, dims, spread, reach, shards=(), kind=jnp.bfloat16):
    loudness = shard_levels(stream_key, dims, shards, -0.22, 0.18) if shards else 1.0
    entries = jax.random.normal(stream_key, dims, jnp.float32) * spread * loudness
    return jnp.minimum(jnp.maximum(entries, -reach), reach).astype(kind)


def setup_inputs(seed: int = 0, part: int = 0) -> dict:
    key_list = jax.random.split(jax.random.key(seed), 13)
    part_splits = jax.random.split(jax.random.fold_in(key_list[12], part), 13)
    tokens = gaussian(part_splits[0], (SEQS, D), 1.0, 6.0, ((1, 4),))
    norm_gain = jnp.clip(1.0 + 0.18 * jax.random.normal(key_list[1], (BLOCKS, D), jnp.float32), 0.1, 1.9)
    w_query = gaussian(key_list[2], (BLOCKS, D, INNER), D ** -0.5, 0.09375, ((1, 4), (2, 4)))
    w_key = gaussian(key_list[3], (BLOCKS, D, INNER), D ** -0.5, 0.09375, ((1, 4), (2, 4)))
    w_value = gaussian(key_list[4], (BLOCKS, D, INNER), D ** -0.5, 0.09375, ((1, 4), (2, 4)))
    w_outgate = gaussian(key_list[5], (BLOCKS, D, INNER), D ** -0.5, 0.09375, ((1, 4), (2, 4)))
    gate_weight = gaussian(key_list[6], (BLOCKS, HEADS, 3 * DK, 2), (3 * DK) ** -0.5, 0.3125, ((1, 4),))
    forget_bias = jnp.clip(-2.0 + 6.0 * jax.random.uniform(key_list[7], (BLOCKS, HEADS), jnp.float32) ** shard_levels(key_list[7], (BLOCKS, HEADS), ((1, 4),), -0.2, 0.2), -2.0, 4.0)
    w_mix = gaussian(key_list[8], (BLOCKS, INNER, D), INNER ** -0.5, 0.25, ((1, 4), (2, 4)))
    memory = gaussian(part_splits[9], (BLOCKS, SEQS, HEADS, DK, DK), 0.3, 3.0, ((1, 4), (2, 4)), jnp.float32)
    normalizer = gaussian(part_splits[10], (BLOCKS, SEQS, HEADS, DK), 0.3, 3.0, ((1, 4), (2, 4)), jnp.float32)
    stabilizer = gaussian(part_splits[11], (BLOCKS, SEQS, HEADS), 1.0, 4.0, ((1, 4), (2, 4)), jnp.float32)
    return dict(tokens=tokens, norm_gain=norm_gain, w_query=w_query, w_key=w_key, w_value=w_value, w_outgate=w_outgate, gate_weight=gate_weight, forget_bias=forget_bias, w_mix=w_mix, memory=memory, normalizer=normalizer, stabilizer=stabilizer)


EPS = 1e-06

def reference(tokens, norm_gain, w_query, w_key, w_value, w_outgate, gate_weight, forget_bias, w_mix, memory, normalizer, stabilizer):
    x = tokens
    mems, norms, stabs = ([], [], [])
    seqs = tokens.shape[0]
    for blk in range(BLOCKS):
        xf = x.astype(jnp.float32)
        squares = lax.optimization_barrier(jnp.sum(xf * xf, axis=-1))
        scale = lax.rsqrt(squares / D + EPS)
        scaled_in = (xf * norm_gain[blk]).astype(jnp.bfloat16)
        projs = []
        for weight in (w_query, w_key, w_value, w_outgate):
            prod = jnp.dot(scaled_in, weight[blk], preferred_element_type=jnp.float32)
            projs.append((scale[:, None] * prod).astype(jnp.bfloat16).astype(jnp.float32).reshape(seqs, HEADS, DK))
        query, key, value, outgate = projs
        joined = jnp.concatenate([query, key, value], axis=-1)
        pre = jnp.einsum('shc,hcg->shg', joined, gate_weight[blk].astype(jnp.float32), precision=lax.Precision.HIGHEST)
        log_input = pre[..., 0]
        log_forget = jax.nn.log_sigmoid(pre[..., 1] + forget_bias[blk])
        stab = stabilizer[blk]
        new_stab = jnp.maximum(log_forget + stab, log_input)
        keep = jnp.exp(log_forget + stab - new_stab)
        admit = jnp.exp(log_input - new_stab)
        scaled_key = key * DK ** (-0.5)
        new_mem = keep[..., None, None] * memory[blk] + admit[..., None, None] * scaled_key[..., :, None] * value[..., None, :]
        new_norm = keep[..., None] * normalizer[blk] + admit[..., None] * scaled_key
        numer = jnp.einsum('shd,shde->she', query, new_mem, precision=lax.Precision.HIGHEST)
        denom = jnp.maximum(jnp.abs(lax.optimization_barrier(jnp.sum(query * new_norm, axis=-1))), 1.0)
        readout = numer / denom[..., None]
        gated = (readout * jax.nn.sigmoid(outgate)).reshape(seqs, HEADS * DK).astype(jnp.bfloat16)
        mixed = jnp.dot(gated, w_mix[blk], preferred_element_type=jnp.float32)
        x = (xf + mixed).astype(jnp.bfloat16)
        mems.append(new_mem)
        norms.append(new_norm)
        stabs.append(new_stab)
    return (x, jnp.stack(mems, axis=0), jnp.stack(norms, axis=0), jnp.stack(stabs, axis=0))
```

```python
import functools

import jax
import jax.numpy as jnp
from jax import lax
from jax.experimental import pallas as pl
from jax.experimental.pallas import tpu as pltpu
from jax.sharding import PartitionSpec as P

EPS = 1e-06
F32 = jnp.float32
BF16 = jnp.bfloat16
MESH = pl.DeviceIdType.MESH


def step_kernel(
    n, m, features,
    tokens, gain, w_query, w_key, w_value, w_outgate, gate_w, w_mix, memory, normalizer, stabilizer, bias,
    x_out, keep_out, value_out, key_out, norm_out, stab_out,
    gain_v, w_v, gate_v, mix_v, mem_v, norm_v, stab_v,
    x_v, xf_v, part_send, part_own, part_recv, gated_v, mix_f, mix_send, mix_own, mix_recv,
    load_sem, ps_sem, pr_sem, gs_sem, gr_sem, ms_sem, mr_sem, xs_sem, xr_sem,
):
    blocks = memory.shape[0]
    own, heads, dk = memory.shape[1], memory.shape[2], memory.shape[3]
    rows = x_v.shape[2]
    width = heads * dk
    dp, tp = lax.axis_index("dp"), lax.axis_index("tp")

    def load(k, src, dst):
        return pltpu.make_async_copy(src, dst, load_sem.at[k])

    loads = {}
    order = [("x", 0, tokens, x_v.at[0]), ("g", 0, gain, gain_v)]
    for b in range(blocks):
        for k, w in enumerate((w_query, w_key, w_value, w_outgate)):
            order.append((f"w{k}", b, w.at[b], w_v.at[b, :, pl.ds(k * width, width)]))
        if b == 0:
            order.append(("gate", 0, gate_w, gate_v))
            order.append(("norm", 0, normalizer, norm_v))
            order.append(("stab", 0, stabilizer, stab_v))
        order.append(("mem", b, memory.at[b], mem_v.at[b]))
        order.append(("mix", b, w_mix.at[b], mix_v.at[b]))
    for k, (name, b, src, dst) in enumerate(order):
        loads[name, b] = load(k, src, dst)
        loads[name, b].start()

    barrier = pltpu.get_barrier_semaphore()
    for o in range(1, n):
        pl.semaphore_signal(barrier, inc=1, device_id={"dp": lax.rem(dp + o, n)}, device_id_type=MESH)
    for o in range(1, m):
        pl.semaphore_signal(barrier, inc=1, device_id={"tp": lax.rem(tp + o, m)}, device_id_type=MESH)

    def send(src, dst, s_sem, r_sem, axis, size, me, o):
        return pltpu.make_async_remote_copy(
            src_ref=src, dst_ref=dst, send_sem=s_sem, recv_sem=r_sem,
            device_id={axis: lax.rem(me + o, size)}, device_id_type=MESH,
        )

    sent = []
    loads["x", 0].wait()
    loads["g", 0].wait()
    for b in range(blocks):
        for j in range(m):
            xf_v[j * rows:(j + 1) * rows, :] = x_v[b, j].astype(F32)
        xf = xf_v[...]
        squares = jnp.sum(xf * xf, axis=-1, keepdims=True)
        scaled_in = (xf * gain_v[b:b + 1, :]).astype(BF16)
        for k in range(4):
            loads[f"w{k}", b].wait()
        part = jnp.dot(scaled_in, w_v[b], preferred_element_type=F32)
        lane = lax.broadcasted_iota(jnp.int32, (own, 128), 1)
        for j in range(n):
            piece = part[j * own:(j + 1) * own, :]
            sq = jnp.broadcast_to(squares[j * own:(j + 1) * own, :], (own, 128))
            high = sq.astype(BF16)
            low = (sq - high.astype(F32)).astype(BF16)
            part_send[b, j, :, : 4 * width] = piece.astype(BF16)
            part_send[b, j, :, 4 * width:] = jnp.where(lane < 64, high.astype(F32), low.astype(F32)).astype(BF16)
            part_own[j, :, : 4 * width] = piece
            part_own[j, :, 4 * width:] = jnp.where(lane < 64, sq, 0.0)
        if b == 0:
            pl.semaphore_wait(barrier, n - 1 + m - 1)
        copies = []
        for o in range(1, n):
            to = lax.rem(dp + o, n)
            c = send(part_send.at[b, to], part_recv.at[b, o - 1], ps_sem.at[b, o - 1], pr_sem.at[b, o - 1], "dp", n, dp, o)
            c.start()
            copies.append(c)
        total = part_own[dp]
        for o, c in enumerate(copies):
            c.wait_recv()
            total = total + part_recv[b, o].astype(F32)
        sent += copies
        own_sq = total[:, 4 * width:4 * width + 1] + total[:, 4 * width + 64:4 * width + 65]
        scale = lax.rsqrt(own_sq / features + EPS)
        projs = (scale * total[:, : 4 * width]).astype(BF16)
        if b == 0:
            loads["gate", 0].wait()
            loads["norm", 0].wait()
            loads["stab", 0].wait()
        loads["mem", b].wait()
        for h in range(heads):
            q16, k16, v16, o16 = (projs[:, k * width + h * dk:k * width + (h + 1) * dk] for k in range(4))
            query, key, value, outgate = (t.astype(F32) for t in (q16, k16, v16, o16))
            pre = (
                jnp.dot(q16, gate_v[b, h, :dk], preferred_element_type=F32)
                + jnp.dot(k16, gate_v[b, h, dk:2 * dk], preferred_element_type=F32)
                + jnp.dot(v16, gate_v[b, h, 2 * dk:], preferred_element_type=F32)
            )
            log_input = pre[:, 0:1]
            z = pre[:, 1:2] + bias[b, h]
            log_forget = jnp.minimum(z, 0.0) - jnp.log1p(jnp.exp(-jnp.abs(z)))
            stab = stab_v[b, :, h:h + 1]
            new_stab = jnp.maximum(log_forget + stab, log_input)
            keep = jnp.exp(log_forget + stab - new_stab)
            admit = jnp.exp(log_input - new_stab)
            ak = admit * (key * dk ** (-0.5))
            new_norm = keep * norm_v[b, :, h, :] + ak
            query_t = query.T
            held = jnp.concatenate(
                [jnp.sum(query_t[:, s:s + 1] * mem_v[b, s, h], axis=0, keepdims=True) for s in range(own)], axis=0
            )
            numer = keep * held + jnp.sum(query * ak, axis=-1, keepdims=True) * value
            denom = jnp.maximum(jnp.abs(jnp.sum(query * new_norm, axis=-1, keepdims=True)), 1.0)
            gated_v[b, dp, :, h * dk:(h + 1) * dk] = (numer / denom * jax.nn.sigmoid(outgate)).astype(BF16)
            stab_out[b, :, h:h + 1] = new_stab
            norm_out[b, :, h, :] = new_norm
            keep_out[b, h] = jnp.broadcast_to(keep, (own, dk))
            value_out[b, h] = value
            key_out[b, h] = ak.T
        copies = []
        for o in range(1, n):
            c = send(gated_v.at[b, dp], gated_v.at[b, dp], gs_sem.at[b, o - 1], gr_sem.at[b, o - 1], "dp", n, dp, o)
            c.start()
            copies.append(c)
        loads["mix", b].wait()
        for c in copies:
            c.wait_recv()
        sent += copies
        every = gated_v[b].reshape(n * own, width)
        mix_f[...] = jnp.dot(every, mix_v[b], preferred_element_type=F32)
        for j in range(m):
            piece = mix_f[j * rows:(j + 1) * rows, :]
            mix_send[b, j] = piece.astype(BF16)
            mix_own[j] = piece
        copies = []
        for o in range(1, m):
            to = lax.rem(tp + o, m)
            c = send(mix_send.at[b, to], mix_recv.at[b, o - 1], ms_sem.at[b, o - 1], mr_sem.at[b, o - 1], "tp", m, tp, o)
            c.start()
            copies.append(c)
        total = mix_own[tp]
        for o, c in enumerate(copies):
            c.wait_recv()
            total = total + mix_recv[b, o].astype(F32)
        sent += copies
        x_v[b + 1, tp] = (x_v[b, tp].astype(F32) + total).astype(BF16)
        copies = []
        for o in range(1, m):
            c = send(x_v.at[b + 1, tp], x_v.at[b + 1, tp], xs_sem.at[b, o - 1], xr_sem.at[b, o - 1], "tp", m, tp, o)
            c.start()
            copies.append(c)
        for c in copies:
            c.wait_recv()
        sent += copies
    x_out[...] = x_v[blocks]
    for c in sent:
        c.wait_send()


def state_kernel(memory, keep, value, key, x, norm, stab, new_memory, x_out, norm_out, stab_out):
    own, heads = memory.shape[1], memory.shape[2]
    for h in range(heads):
        keys = key[0, h]
        for s in range(own):
            new_memory[0, s, h] = (
                keep[0, h, s:s + 1, :] * memory[0, s, h] + keys[:, s:s + 1] * value[0, h, s:s + 1, :]
            )
    x_out[...] = x[...]
    norm_out[...] = norm[...]
    stab_out[...] = stab[...]


def shards(n, m, tokens, norm_gain, w_query, w_key, w_value, w_outgate, gate_weight, forget_bias, w_mix, memory, normalizer, stabilizer):
    seqs, feats = tokens.shape
    blocks, own, heads, dk, _ = memory.shape
    width = heads * dk
    rows = seqs // m
    cols = 4 * width + 128
    anywhere = pl.BlockSpec(memory_space=pl.ANY)
    vmem = pl.BlockSpec(memory_space=pltpu.VMEM)
    dma = pltpu.SemaphoreType.DMA
    nd, nt = max(n - 1, 1), max(m - 1, 1)
    sds = jax.ShapeDtypeStruct
    x, keep, value, key, norm, stab = pl.pallas_call(
        functools.partial(step_kernel, n, m, n * feats),
        out_shape=(
            sds((m, rows, feats), BF16),
            sds((blocks, heads, own, dk), F32),
            sds((blocks, heads, own, dk), F32),
            sds((blocks, heads, dk, own), F32),
            sds((blocks, own, heads, dk), F32),
            sds((blocks, own, heads), F32),
        ),
        in_specs=[anywhere] * 11 + [pl.BlockSpec(memory_space=pltpu.SMEM)],
        out_specs=(vmem,) * 6,
        scratch_shapes=[
            pltpu.VMEM(norm_gain.shape, F32),
            pltpu.VMEM((blocks, feats, 4 * width), BF16),
            pltpu.VMEM(gate_weight.shape, BF16),
            pltpu.VMEM(w_mix.shape, BF16),
            pltpu.VMEM(memory.shape, F32),
            pltpu.VMEM(normalizer.shape, F32),
            pltpu.VMEM(stabilizer.shape, F32),
            pltpu.VMEM((blocks + 1, m, rows, feats), BF16),
            pltpu.VMEM((seqs, feats), F32),
            pltpu.VMEM((blocks, n, own, cols), BF16),
            pltpu.VMEM((n, own, cols), F32),
            pltpu.VMEM((blocks, nd, own, cols), BF16),
            pltpu.VMEM((blocks, n, own, width), BF16),
            pltpu.VMEM((seqs, feats), F32),
            pltpu.VMEM((blocks, m, rows, feats), BF16),
            pltpu.VMEM((m, rows, feats), F32),
            pltpu.VMEM((blocks, nt, rows, feats), BF16),
            dma((5 + 6 * blocks,)),
            dma((blocks, nd)), dma((blocks, nd)), dma((blocks, nd)), dma((blocks, nd)),
            dma((blocks, nt)), dma((blocks, nt)), dma((blocks, nt)), dma((blocks, nt)),
        ],
        compiler_params=pltpu.CompilerParams(collective_id=0, has_side_effects=True),
    )(
        tokens.reshape(m, rows, feats), norm_gain, w_query, w_key, w_value, w_outgate,
        gate_weight, w_mix, memory, normalizer, stabilizer, forget_bias,
    )

    def per_block(shape):
        return pl.BlockSpec((1,) + shape[1:], lambda b: (b,) + (0,) * (len(shape) - 1))

    def whole(shape):
        return pl.BlockSpec(shape, lambda b: (0,) * len(shape))

    new_memory, x, norm, stab = pl.pallas_call(
        state_kernel,
        grid=(blocks,),
        out_shape=(sds(memory.shape, F32), sds(x.shape, BF16), sds(norm.shape, F32), sds(stab.shape, F32)),
        in_specs=[per_block(t.shape) for t in (memory, keep, value, key)] + [whole(t.shape) for t in (x, norm, stab)],
        out_specs=(per_block(memory.shape), whole(x.shape), whole(norm.shape), whole(stab.shape)),
    )(memory, keep, value, key, x, norm, stab)
    return x.reshape(seqs, feats), new_memory, norm, stab


def solution(mesh):
    in_specs = (
        P("grp", "dp"),
        P(None, "dp"),
        P(None, "dp", "tp"),
        P(None, "dp", "tp"),
        P(None, "dp", "tp"),
        P(None, "dp", "tp"),
        P(None, "tp", None, None),
        P(None, "tp"),
        P(None, "tp", "dp"),
        P(None, ("grp", "dp"), "tp", None, None),
        P(None, ("grp", "dp"), "tp", None),
        P(None, ("grp", "dp"), "tp"),
    )
    out_specs = (
        P("grp", "dp"),
        P(None, ("grp", "dp"), "tp", None, None),
        P(None, ("grp", "dp"), "tp", None),
        P(None, ("grp", "dp"), "tp"),
    )
    body = functools.partial(shards, mesh.shape["dp"], mesh.shape["tp"])
    return jax.shard_map(body, mesh=mesh, in_specs=in_specs, out_specs=out_specs, check_vma=False)
```

```python
import functools

import jax
import jax.numpy as jnp
from jax import lax
from jax.experimental import pallas as pl
from jax.experimental.pallas import tpu as pltpu
from jax.sharding import PartitionSpec as P

EPS = 1e-06
F32 = jnp.float32
BF16 = jnp.bfloat16
MESH = pl.DeviceIdType.MESH


def step_kernel(
    n, m, features,
    tokens, gain, w_query, w_key, w_value, w_outgate, gate_w, w_mix, memory, normalizer, stabilizer, bias,
    x_out, keep_out, value_out, key_out, norm_out, stab_out,
    gain_v, w_v, gate_v, mix_v, mem_v, norm_v, stab_v,
    x_v, xf_v, part_send, part_own, part_recv, gated_v, mix_f, mix_send, mix_own, mix_recv,
    load_sem, ps_sem, pr_sem, gs_sem, gr_sem, ms_sem, mr_sem, xs_sem, xr_sem,
):
    blocks = memory.shape[0]
    own, heads, dk = memory.shape[1], memory.shape[2], memory.shape[3]
    rows = x_v.shape[2]
    width = heads * dk
    dp, tp = lax.axis_index("dp"), lax.axis_index("tp")

    def load(k, src, dst):
        return pltpu.make_async_copy(src, dst, load_sem.at[k])

    loads = {}
    order = [("x", 0, tokens, x_v.at[0]), ("g", 0, gain, gain_v)]
    for b in range(blocks):
        for k, w in enumerate((w_query, w_key, w_value, w_outgate)):
            order.append((f"w{k}", b, w.at[b], w_v.at[b, :, pl.ds(k * width, width)]))
        if b == 0:
            order.append(("gate", 0, gate_w, gate_v))
            order.append(("norm", 0, normalizer, norm_v))
            order.append(("stab", 0, stabilizer, stab_v))
        order.append(("mem", b, memory.at[b], mem_v.at[b]))
        order.append(("mix", b, w_mix.at[b], mix_v.at[b]))
    for k, (name, b, src, dst) in enumerate(order):
        loads[name, b] = load(k, src, dst)
        loads[name, b].start()

    barrier = pltpu.get_barrier_semaphore()
    for o in range(1, n):
        pl.semaphore_signal(barrier, inc=1, device_id={"dp": lax.rem(dp + o, n)}, device_id_type=MESH)
    for o in range(1, m):
        pl.semaphore_signal(barrier, inc=1, device_id={"tp": lax.rem(tp + o, m)}, device_id_type=MESH)

    def send(src, dst, s_sem, r_sem, axis, size, me, o):
        return pltpu.make_async_remote_copy(
            src_ref=src, dst_ref=dst, send_sem=s_sem, recv_sem=r_sem,
            device_id={axis: lax.rem(me + o, size)}, device_id_type=MESH,
        )

    sent = []
    diagonal = lax.broadcasted_iota(jnp.int32, (own, own), 0) == lax.broadcasted_iota(jnp.int32, (own, own), 1)
    loads["x", 0].wait()
    loads["g", 0].wait()
    for b in range(blocks):
        for j in range(m):
            xf_v[j * rows:(j + 1) * rows, :] = x_v[b, j].astype(F32)
        xf = xf_v[...]
        squares = jnp.sum(xf * xf, axis=-1, keepdims=True)
        scaled_in = (xf * gain_v[b:b + 1, :]).astype(BF16)
        for k in range(4):
            loads[f"w{k}", b].wait()
        part = jnp.dot(scaled_in, w_v[b], preferred_element_type=F32)
        lane = lax.broadcasted_iota(jnp.int32, (own, 128), 1)
        for j in range(n):
            piece = part[j * own:(j + 1) * own, :]
            sq = jnp.broadcast_to(squares[j * own:(j + 1) * own, :], (own, 128))
            high = sq.astype(BF16)
            low = (sq - high.astype(F32)).astype(BF16)
            part_send[b, j, :, : 4 * width] = piece.astype(BF16)
            part_send[b, j, :, 4 * width:] = jnp.where(lane < 64, high.astype(F32), low.astype(F32)).astype(BF16)
            part_own[j, :, : 4 * width] = piece
            part_own[j, :, 4 * width:] = jnp.where(lane < 64, sq, 0.0)
        if b == 0:
            pl.semaphore_wait(barrier, n - 1 + m - 1)
        copies = []
        for o in range(1, n):
            to = lax.rem(dp + o, n)
            c = send(part_send.at[b, to], part_recv.at[b, o - 1], ps_sem.at[b, o - 1], pr_sem.at[b, o - 1], "dp", n, dp, o)
            c.start()
            copies.append(c)
        total = part_own[dp]
        for o, c in enumerate(copies):
            c.wait_recv()
            total = total + part_recv[b, o].astype(F32)
        sent += copies
        own_sq = total[:, 4 * width:4 * width + 1] + total[:, 4 * width + 64:4 * width + 65]
        scale = lax.rsqrt(own_sq / features + EPS)
        projs = (scale * total[:, : 4 * width]).astype(BF16)
        if b == 0:
            loads["gate", 0].wait()
            loads["norm", 0].wait()
            loads["stab", 0].wait()
        loads["mem", b].wait()
        for h in range(heads):
            query, key, value, outgate = (
                projs[:, k * width + h * dk:k * width + (h + 1) * dk].astype(F32) for k in range(4)
            )
            gate = gate_v[b, h].astype(F32)

            def pre(g):
                terms = (
                    query * gate[g:g + 1, :dk] + key * gate[g:g + 1, dk:2 * dk] + value * gate[g:g + 1, 2 * dk:]
                )
                return jnp.sum(terms, axis=-1, keepdims=True)

            log_input = pre(0)
            z = pre(1) + bias[h, b]
            log_forget = jnp.minimum(z, 0.0) - jnp.log1p(jnp.exp(-jnp.abs(z)))
            stab = jnp.sum(jnp.where(diagonal, stab_v[b, h:h + 1, :], 0.0), axis=1, keepdims=True)
            new_stab = jnp.maximum(log_forget + stab, log_input)
            keep = jnp.exp(log_forget + stab - new_stab)
            admit = jnp.exp(log_input - new_stab)
            ak = admit * (key * dk ** (-0.5))
            new_norm = keep * norm_v[b, :, h * dk:(h + 1) * dk] + ak
            query_t = query.T
            held = jnp.concatenate(
                [jnp.sum(query_t[:, s:s + 1] * mem_v[b, s, h], axis=0, keepdims=True) for s in range(own)], axis=0
            )
            numer = keep * held + jnp.sum(query * ak, axis=-1, keepdims=True) * value
            denom = jnp.maximum(jnp.abs(jnp.sum(query * new_norm, axis=-1, keepdims=True)), 1.0)
            gated_v[b, dp, :, h * dk:(h + 1) * dk] = (numer / denom * jax.nn.sigmoid(outgate)).astype(BF16)
            stab_out[b, h:h + 1, :] = jnp.sum(jnp.where(diagonal, new_stab, 0.0), axis=0, keepdims=True)
            norm_out[b, :, h * dk:(h + 1) * dk] = new_norm
            keep_out[b, h] = jnp.broadcast_to(keep, (own, dk))
            value_out[b, h] = value
            key_out[b, h] = ak.T
        copies = []
        for o in range(1, n):
            c = send(gated_v.at[b, dp], gated_v.at[b, dp], gs_sem.at[b, o - 1], gr_sem.at[b, o - 1], "dp", n, dp, o)
            c.start()
            copies.append(c)
        loads["mix", b].wait()
        for c in copies:
            c.wait_recv()
        sent += copies
        every = gated_v[b].reshape(n * own, width)
        mix_f[...] = jnp.dot(every, mix_v[b], preferred_element_type=F32)
        for j in range(m):
            piece = mix_f[j * rows:(j + 1) * rows, :]
            mix_send[b, j] = piece.astype(BF16)
            mix_own[j] = piece
        copies = []
        for o in range(1, m):
            to = lax.rem(tp + o, m)
            c = send(mix_send.at[b, to], mix_recv.at[b, o - 1], ms_sem.at[b, o - 1], mr_sem.at[b, o - 1], "tp", m, tp, o)
            c.start()
            copies.append(c)
        total = mix_own[tp]
        for o, c in enumerate(copies):
            c.wait_recv()
            total = total + mix_recv[b, o].astype(F32)
        sent += copies
        x_v[b + 1, tp] = (x_v[b, tp].astype(F32) + total).astype(BF16)
        copies = []
        for o in range(1, m):
            c = send(x_v.at[b + 1, tp], x_v.at[b + 1, tp], xs_sem.at[b, o - 1], xr_sem.at[b, o - 1], "tp", m, tp, o)
            c.start()
            copies.append(c)
        for c in copies:
            c.wait_recv()
        sent += copies
    x_out[...] = x_v[blocks]
    for c in sent:
        c.wait_send()


def state_kernel(memory, keep, value, key, x, norm, stab, new_memory, x_out, norm_out, stab_out):
    own, heads = memory.shape[1], memory.shape[2]
    for h in range(heads):
        keys = key[0, h]
        for s in range(own):
            new_memory[0, s, h] = (
                keep[0, h, s:s + 1, :] * memory[0, s, h] + keys[:, s:s + 1] * value[0, h, s:s + 1, :]
            )
    x_out[...] = x[...]
    norm_out[...] = norm[...]
    stab_out[...] = stab[...]


def shards(n, m, tokens, norm_gain, w_query, w_key, w_value, w_outgate, gate_weight, forget_bias, w_mix, memory, normalizer, stabilizer):
    seqs, feats = tokens.shape
    blocks, own, heads, dk, _ = memory.shape
    width = heads * dk
    rows = seqs // m
    cols = 4 * width + 128
    anywhere = pl.BlockSpec(memory_space=pl.ANY)
    vmem = pl.BlockSpec(memory_space=pltpu.VMEM)
    dma = pltpu.SemaphoreType.DMA
    nd, nt = max(n - 1, 1), max(m - 1, 1)
    sds = jax.ShapeDtypeStruct
    x, keep, value, key, norm, stab = pl.pallas_call(
        functools.partial(step_kernel, n, m, n * feats),
        out_shape=(
            sds((m, rows, feats), BF16),
            sds((blocks, heads, own, dk), F32),
            sds((blocks, heads, own, dk), F32),
            sds((blocks, heads, dk, own), F32),
            sds((blocks, own, width), F32),
            sds((blocks, heads, own), F32),
        ),
        in_specs=[anywhere] * 11 + [pl.BlockSpec(memory_space=pltpu.SMEM)],
        out_specs=(vmem,) * 6,
        scratch_shapes=[
            pltpu.VMEM(norm_gain.shape, F32),
            pltpu.VMEM((blocks, feats, 4 * width), BF16),
            pltpu.VMEM((blocks, heads, 2, 3 * dk), BF16),
            pltpu.VMEM(w_mix.shape, BF16),
            pltpu.VMEM(memory.shape, F32),
            pltpu.VMEM((blocks, own, width), F32),
            pltpu.VMEM((blocks, heads, own), F32),
            pltpu.VMEM((blocks + 1, m, rows, feats), BF16),
            pltpu.VMEM((seqs, feats), F32),
            pltpu.VMEM((blocks, n, own, cols), BF16),
            pltpu.VMEM((n, own, cols), F32),
            pltpu.VMEM((blocks, nd, own, cols), BF16),
            pltpu.VMEM((blocks, n, own, width), BF16),
            pltpu.VMEM((seqs, feats), F32),
            pltpu.VMEM((blocks, m, rows, feats), BF16),
            pltpu.VMEM((m, rows, feats), F32),
            pltpu.VMEM((blocks, nt, rows, feats), BF16),
            dma((5 + 6 * blocks,)),
            dma((blocks, nd)), dma((blocks, nd)), dma((blocks, nd)), dma((blocks, nd)),
            dma((blocks, nt)), dma((blocks, nt)), dma((blocks, nt)), dma((blocks, nt)),
        ],
        compiler_params=pltpu.CompilerParams(collective_id=0, has_side_effects=True),
    )(
        tokens.reshape(m, rows, feats), norm_gain, w_query, w_key, w_value, w_outgate,
        jnp.swapaxes(gate_weight, 2, 3), w_mix, memory, normalizer.reshape(blocks, own, width),
        jnp.swapaxes(stabilizer, 1, 2), forget_bias.T,
    )

    def per_block(shape):
        return pl.BlockSpec((1,) + shape[1:], lambda b: (b,) + (0,) * (len(shape) - 1))

    def whole(shape):
        return pl.BlockSpec(shape, lambda b: (0,) * len(shape))

    new_memory, x, norm, stab = pl.pallas_call(
        state_kernel,
        grid=(blocks,),
        out_shape=(sds(memory.shape, F32), sds(x.shape, BF16), sds(norm.shape, F32), sds(stab.shape, F32)),
        in_specs=[per_block(t.shape) for t in (memory, keep, value, key)] + [whole(t.shape) for t in (x, norm, stab)],
        out_specs=(per_block(memory.shape), whole(x.shape), whole(norm.shape), whole(stab.shape)),
    )(memory, keep, value, key, x, norm, stab)
    return x.reshape(seqs, feats), new_memory, norm.reshape(normalizer.shape), jnp.swapaxes(stab, 1, 2)


def solution(mesh):
    in_specs = (
        P("grp", "dp"),
        P(None, "dp"),
        P(None, "dp", "tp"),
        P(None, "dp", "tp"),
        P(None, "dp", "tp"),
        P(None, "dp", "tp"),
        P(None, "tp", None, None),
        P(None, "tp"),
        P(None, "tp", "dp"),
        P(None, ("grp", "dp"), "tp", None, None),
        P(None, ("grp", "dp"), "tp", None),
        P(None, ("grp", "dp"), "tp"),
    )
    out_specs = (
        P("grp", "dp"),
        P(None, ("grp", "dp"), "tp", None, None),
        P(None, ("grp", "dp"), "tp", None),
        P(None, ("grp", "dp"), "tp"),
    )
    body = functools.partial(shards, mesh.shape["dp"], mesh.shape["tp"])
    return jax.shard_map(body, mesh=mesh, in_specs=in_specs, out_specs=out_specs, check_vma=False)
```

```python
import functools

import jax
import jax.numpy as jnp
from jax import lax
from jax.experimental import pallas as pl
from jax.experimental.pallas import tpu as pltpu
from jax.sharding import PartitionSpec as P

EPS = 1e-06
F32 = jnp.float32
BF16 = jnp.bfloat16
MESH = pl.DeviceIdType.MESH


def step_kernel(
    sizes, fast,
    tokens, gain, w_query, w_key, w_value, w_outgate, gate_w, w_mix, memory, normalizer, stabilizer, bias,
    x_out, memory_out, norm_out, stab_out,
    gain_v, w_v, gate_v, mix_v, mixcol_v, mem_v, norm_v, stab_v, tokens_v, xf_v, part_send, part_own, part_recv,
    gated_v, xcol_v, mix_send, mix_own, mix_recv, xrow_v,
    load_sem, ps_sem, pr_sem, gs_sem, gr_sem, ms_sem, mr_sem, xs_sem, xr_sem, zs_sem, zr_sem, ys_sem, yr_sem,
):
    groups, n, m = sizes
    blocks = memory.shape[0]
    own, heads, dk = memory.shape[1], memory.shape[2], memory.shape[3]
    seqs, feats = tokens.shape
    features = n * feats
    rows, cols = seqs // m, feats // m
    width = heads * dk
    share = width // groups
    grp, dp, tp = lax.axis_index("grp"), lax.axis_index("dp"), lax.axis_index("tp")
    last = blocks - 1

    def mix_slot(b, t):
        return mix_v.at[t] if b == last else mixcol_v.at[b, t]

    def mix_cols(b, to):
        return pl.ds(0, feats) if b == last else pl.ds(pl.multiple_of(to * cols, cols), cols)

    order = [("x", 0, tokens, tokens_v), ("g", 0, gain, gain_v)]
    for b in range(blocks):
        for k, w in enumerate((w_query, w_key, w_value, w_outgate)):
            order.append((f"w{k}", b, w.at[b], w_v.at[b, :, pl.ds(k * width, width)]))
        if b == 0:
            order.append(("gate", 0, gate_w, gate_v))
            order.append(("norm", 0, normalizer, norm_v))
            order.append(("stab", 0, stabilizer, stab_v))
        order.append(("mem", b, memory.at[b], mem_v.at[b]))
        if fast:
            order.append(("mix", b, w_mix.at[b, :, mix_cols(b, tp)], mix_slot(b, tp)))
        else:
            order.append(("mix", b, w_mix.at[b], mix_v.at[b]))
    loads = {}
    for k, (name, b, src, dst) in enumerate(order):
        loads[name, b] = pltpu.make_async_copy(src, dst, load_sem.at[k])
        loads[name, b].start()

    if fast:
        peers = [(od, ot) for ot in range(m) for od in range(n) if (od, ot) != (0, 0)]
    else:
        peers = [(od, 0) for od in range(1, n)] + [(0, ot) for ot in range(1, m)]
    barrier = pltpu.get_barrier_semaphore()

    def at(od, ot, og=0):
        return {"grp": lax.rem(grp + og, groups), "dp": lax.rem(dp + od, n), "tp": lax.rem(tp + ot, m)}

    for od, ot in peers:
        pl.semaphore_signal(barrier, inc=1, device_id=at(od, ot), device_id_type=MESH)
    greeted = len(peers)
    if fast:
        for og in range(1, groups):
            pl.semaphore_signal(barrier, inc=1, device_id=at(0, 0, og), device_id_type=MESH)
        greeted += groups - 1

    sent = []

    def send(src, dst, s_sem, r_sem, where):
        c = pltpu.make_async_remote_copy(
            src_ref=src, dst_ref=dst, send_sem=s_sem, recv_sem=r_sem, device_id=where, device_id_type=MESH
        )
        c.start()
        sent.append(c)
        return c

    def spread(b, offsets):
        part = pl.ds(pl.multiple_of(grp * share, share), share)
        return [
            (o, send(w_mix.at[b, part, mix_cols(b, lax.rem(tp + o, m))], mix_slot(b, tp).at[part],
                     zs_sem.at[b, o - 1], zr_sem.at[b, o - 1], at(0, o)))
            for o in offsets
        ]

    def relay(b, arriving):
        part = pl.ds(pl.multiple_of(grp * share, share), share)
        out = []
        for o, c in arriving:
            c.wait_recv()
            ref = mix_slot(b, lax.rem(tp + m - o, m)).at[part]
            for og in range(1, groups):
                out.append(send(ref, ref, ys_sem.at[b, o - 1, og - 1], yr_sem.at[b, o - 1, og - 1], at(0, 0, og)))
        return out

    diagonal = lax.broadcasted_iota(jnp.int32, (own, own), 0) == lax.broadcasted_iota(jnp.int32, (own, own), 1)
    lane = lax.broadcasted_iota(jnp.int32, (own, 128), 1)
    pending, relayed = {b: [] for b in range(blocks)}, {b: [] for b in range(blocks)}
    loads["x", 0].wait()
    loads["g", 0].wait()
    xf_v[...] = tokens_v[...].astype(F32)
    for b in range(blocks):
        xf = xf_v[...]
        squares = jnp.sum(xf * xf, axis=-1, keepdims=True)
        scaled_in = (xf * gain_v[b:b + 1, :]).astype(BF16)
        if b == 0:
            pl.semaphore_wait(barrier, greeted)
            if fast:
                pending[0] = spread(0, range(1, m))
        for k in range(4):
            loads[f"w{k}", b].wait()
        part = jnp.dot(scaled_in, w_v[b], preferred_element_type=F32)
        for j in range(n):
            piece = part[j * own:(j + 1) * own, :]
            sq = jnp.broadcast_to(squares[j * own:(j + 1) * own, :], (own, 128))
            high = sq.astype(BF16)
            low = (sq - high.astype(F32)).astype(BF16)
            part_send[b, j, :, : 4 * width] = piece.astype(BF16)
            part_send[b, j, :, 4 * width:] = jnp.where(lane < 64, high.astype(F32), low.astype(F32)).astype(BF16)
            part_own[j, :, : 4 * width] = piece
            part_own[j, :, 4 * width:] = jnp.where(lane < 64, sq, 0.0)
        copies = [
            send(part_send.at[b, lax.rem(dp + o, n)], part_recv.at[b, o - 1],
                 ps_sem.at[b, o - 1], pr_sem.at[b, o - 1], at(o, 0))
            for o in range(1, n)
        ]
        if b == 0:
            loads["gate", 0].wait()
            loads["norm", 0].wait()
            loads["stab", 0].wait()
        loads["mem", b].wait()
        total = part_own[dp]
        for o, c in enumerate(copies):
            c.wait_recv()
            total = total + part_recv[b, o].astype(F32)
        own_sq = total[:, 4 * width:4 * width + 1] + total[:, 4 * width + 64:4 * width + 65]
        scale = lax.rsqrt(own_sq / features + EPS)
        projs = (scale * total[:, : 4 * width]).astype(BF16)
        mine = gated_v.at[b, tp if fast else 0, dp]
        updates = []
        for h in range(heads):
            query, key, value, outgate = (
                projs[:, k * width + h * dk:k * width + (h + 1) * dk].astype(F32) for k in range(4)
            )
            gate = gate_v[b, h].astype(F32)

            def pre(g):
                terms = (
                    query * gate[g:g + 1, :dk] + key * gate[g:g + 1, dk:2 * dk] + value * gate[g:g + 1, 2 * dk:]
                )
                return jnp.sum(terms, axis=-1, keepdims=True)

            log_input = pre(0)
            z = pre(1) + bias[h, b]
            log_forget = jnp.minimum(z, 0.0) - jnp.log1p(jnp.exp(-jnp.abs(z)))
            stab = jnp.sum(jnp.where(diagonal, stab_v[b, h:h + 1, :], 0.0), axis=1, keepdims=True)
            new_stab = jnp.maximum(log_forget + stab, log_input)
            keep = jnp.exp(log_forget + stab - new_stab)
            admit = jnp.exp(log_input - new_stab)
            ak = admit * (key * dk ** (-0.5))
            new_norm = keep * norm_v[b, :, h * dk:(h + 1) * dk] + ak
            query_t = query.T
            held = jnp.concatenate(
                [jnp.sum(query_t[:, s:s + 1] * mem_v[b, s, h], axis=0, keepdims=True) for s in range(own)], axis=0
            )
            numer = keep * held + jnp.sum(query * ak, axis=-1, keepdims=True) * value
            denom = jnp.maximum(jnp.abs(jnp.sum(query * new_norm, axis=-1, keepdims=True)), 1.0)
            mine[:, h * dk:(h + 1) * dk] = (numer / denom * jax.nn.sigmoid(outgate)).astype(BF16)
            updates.append((keep, ak, value, new_stab, new_norm))
        to = [(od, ot) for ot in reversed(range(m if fast else 1)) for od in range(n) if (od, ot) != (0, 0)]
        copies = [
            send(mine, mine, gs_sem.at[b, ot * n + od], gr_sem.at[b, ot * n + od], at(od, ot)) for od, ot in to
        ]
        if fast:
            if b + 1 == last:
                early = spread(last, range(1, m, 2))
            relayed[b] += relay(b, pending[b])
        for h, (keep, ak, value, new_stab, new_norm) in enumerate(updates):
            stab_out[b, h:h + 1, :] = jnp.sum(jnp.where(diagonal, new_stab, 0.0), axis=0, keepdims=True)
            norm_out[b, :, h * dk:(h + 1) * dk] = new_norm
            ak_t = ak.T
            kept = jnp.broadcast_to(keep, (own, dk))
            for s in range(own):
                memory_out[b, s, h] = kept[s:s + 1, :] * mem_v[b, s, h] + ak_t[:, s:s + 1] * value[s:s + 1, :]
        loads["mix", b].wait()
        for c in copies + relayed[b]:
            c.wait_recv()
        if fast:
            every = jnp.concatenate([gated_v[b, t].reshape(n * own, width) for t in range(m)], axis=1)
        if fast and b == last:
            mixed = jnp.dot(every, mix_v[...].reshape(m * width, feats), preferred_element_type=F32)
            x_out[...] = (xf_v[...] + mixed).astype(BF16)
        elif fast:
            mixed = jnp.dot(every, mixcol_v[b].reshape(m * width, cols), preferred_element_type=F32)
            own_cols = xf_v[:, pl.ds(pl.multiple_of(tp * cols, cols), cols)]
            xcol_v[b, tp] = (own_cols + mixed).astype(BF16)
            ref = xcol_v.at[b, tp]
            copies = [send(ref, ref, xs_sem.at[b, o - 1], xr_sem.at[b, o - 1], at(0, o)) for o in range(1, m)]
            if b + 1 == last:
                pending[last] = spread(last, range(2, m, 2))
                relayed[last] += relay(last, early)
            else:
                pending[b + 1] = spread(b + 1, range(1, m))
            for c in copies:
                c.wait_recv()
            for j in range(m):
                xf_v[:, j * cols:(j + 1) * cols] = xcol_v[b, j].astype(F32)
        else:
            every = gated_v[b, 0].reshape(n * own, width)
            mixed = jnp.dot(every, mix_v[b], preferred_element_type=F32)
            for j in range(m):
                piece = mixed[j * rows:(j + 1) * rows, :]
                mix_send[b, j] = piece.astype(BF16)
                mix_own[j] = piece
                xrow_v[j] = xf_v[j * rows:(j + 1) * rows, :].astype(BF16)
            copies = [
                send(mix_send.at[b, lax.rem(tp + o, m)], mix_recv.at[b, o - 1],
                     ms_sem.at[b, o - 1], mr_sem.at[b, o - 1], at(0, o))
                for o in range(1, m)
            ]
            total = mix_own[tp]
            for o, c in enumerate(copies):
                c.wait_recv()
                total = total + mix_recv[b, o].astype(F32)
            xcol_v[b, tp] = (xrow_v[tp].astype(F32) + total).astype(BF16)
            ref = xcol_v.at[b, tp]
            copies = [send(ref, ref, xs_sem.at[b, o - 1], xr_sem.at[b, o - 1], at(0, o)) for o in range(1, m)]
            for c in copies:
                c.wait_recv()
            for j in range(m):
                xf_v[j * rows:(j + 1) * rows, :] = xcol_v[b, j].astype(F32)
            if b == last:
                x_out[...] = xf_v[...].astype(BF16)
    for c in sent:
        c.wait_send()


def store_kernel(*refs):
    count = (len(refs) - 1) // 2
    sources, results, sem = refs[:count], refs[count:2 * count], refs[-1]
    copies = [pltpu.make_async_copy(a, z, sem.at[k]) for k, (a, z) in enumerate(zip(sources, results))]
    for c in copies:
        c.start()
    for c in copies:
        c.wait()


def shards(sizes, tokens, norm_gain, w_query, w_key, w_value, w_outgate, gate_weight, forget_bias, w_mix, memory, normalizer, stabilizer):
    groups, n, m = sizes
    seqs, feats = tokens.shape
    blocks, own, heads, dk, _ = memory.shape
    width = heads * dk
    rows, cols = seqs // m, feats // m
    wide = 4 * width + 128
    fast = cols % 128 == 0 and width % (16 * groups) == 0 and blocks > 1
    hbm = pl.BlockSpec(memory_space=pltpu.HBM)
    vmem = pl.BlockSpec(memory_space=pltpu.VMEM)
    dma = pltpu.SemaphoreType.DMA
    nd, nt, ng = max(n - 1, 1), max(m - 1, 1), max(groups - 1, 1)
    slow_rows = (1, 8, 128) if fast else (m, rows, feats)
    results = (
        ((seqs, feats), BF16),
        (memory.shape, F32),
        ((blocks, own, width), F32),
        ((blocks, heads, own), F32),
    )
    held = pl.pallas_call(
        functools.partial(step_kernel, sizes, fast),
        out_shape=tuple(pltpu.VMEM(shape, kind) for shape, kind in results),
        in_specs=[hbm] * 11 + [pl.BlockSpec(memory_space=pltpu.SMEM)],
        out_specs=(vmem,) * 4,
        scratch_shapes=[
            pltpu.VMEM(norm_gain.shape, F32),
            pltpu.VMEM((blocks, feats, 4 * width), BF16),
            pltpu.VMEM((blocks, heads, 2, 3 * dk), BF16),
            pltpu.VMEM((m, width, feats) if fast else w_mix.shape, BF16),
            pltpu.VMEM((blocks - 1, m, width, cols) if fast else (1, 1, 16, 128), BF16),
            pltpu.VMEM(memory.shape, F32),
            pltpu.VMEM((blocks, own, width), F32),
            pltpu.VMEM((blocks, heads, own), F32),
            pltpu.VMEM((seqs, feats), BF16),
            pltpu.VMEM((seqs, feats), F32),
            pltpu.VMEM((blocks, n, own, wide), BF16),
            pltpu.VMEM((n, own, wide), F32),
            pltpu.VMEM((blocks, nd, own, wide), BF16),
            pltpu.VMEM((blocks, m if fast else 1, n, own, width), BF16),
            pltpu.VMEM((blocks, m, seqs, cols) if fast else (blocks, m, rows, feats), BF16),
            pltpu.VMEM((blocks,) + slow_rows, BF16),
            pltpu.VMEM(slow_rows, F32),
            pltpu.VMEM((blocks, nt) + slow_rows[1:], BF16),
            pltpu.VMEM(slow_rows, BF16),
            dma((5 + 6 * blocks,)),
            dma((blocks, nd)), dma((blocks, nd)), dma((blocks, n * m)), dma((blocks, n * m)),
            dma((blocks, nt)), dma((blocks, nt)), dma((blocks, nt)), dma((blocks, nt)),
            dma((blocks, nt)), dma((blocks, nt)), dma((blocks, nt, ng)), dma((blocks, nt, ng)),
        ],
        compiler_params=pltpu.CompilerParams(collective_id=0, has_side_effects=True, vmem_limit_bytes=32 << 20),
    )(
        *(
            pltpu.with_memory_space_constraint(t, pltpu.HBM)
            for t in (
                tokens, norm_gain, w_query, w_key, w_value, w_outgate,
                jnp.swapaxes(gate_weight, 2, 3), w_mix, memory, normalizer.reshape(blocks, own, width),
                jnp.swapaxes(stabilizer, 1, 2),
            )
        ),
        forget_bias.T,
    )
    x, new_memory, norm, stab = pl.pallas_call(
        store_kernel,
        out_shape=tuple(jax.ShapeDtypeStruct(shape, kind) for shape, kind in results),
        in_specs=[vmem] * 4,
        out_specs=(pl.BlockSpec(memory_space=pl.ANY),) * 4,
        scratch_shapes=[dma((4,))],
    )(*(pltpu.with_memory_space_constraint(t, pltpu.VMEM) for t in held))
    return x, new_memory, norm.reshape(normalizer.shape), jnp.swapaxes(stab, 1, 2)


def solution(mesh):
    in_specs = (
        P("grp", "dp"),
        P(None, "dp"),
        P(None, "dp", "tp"),
        P(None, "dp", "tp"),
        P(None, "dp", "tp"),
        P(None, "dp", "tp"),
        P(None, "tp", None, None),
        P(None, "tp"),
        P(None, "tp", "dp"),
        P(None, ("grp", "dp"), "tp", None, None),
        P(None, ("grp", "dp"), "tp", None),
        P(None, ("grp", "dp"), "tp"),
    )
    out_specs = (
        P("grp", "dp"),
        P(None, ("grp", "dp"), "tp", None, None),
        P(None, ("grp", "dp"), "tp", None),
        P(None, ("grp", "dp"), "tp"),
    )
    body = functools.partial(shards, (mesh.shape["grp"], mesh.shape["dp"], mesh.shape["tp"]))
    return jax.shard_map(body, mesh=mesh, in_specs=in_specs, out_specs=out_specs, check_vma=False)
```

```python
import functools

import jax
import jax.numpy as jnp
from jax import lax
from jax.experimental import pallas as pl
from jax.experimental.pallas import tpu as pltpu
from jax.sharding import PartitionSpec as P

EPS = 1e-06
F32 = jnp.float32
BF16 = jnp.bfloat16
MESH = pl.DeviceIdType.MESH


def step_kernel(
    sizes, fast,
    tokens, gain, w_query, w_key, w_value, w_outgate, gate_w, w_mix, memory, normalizer, stabilizer, bias_h,
    x_out, memory_out, norm_out, stab_out,
    gain_v, w_v, gate_v, mix_v, mixcol_v, mem_v, norm_v, stab_v, bias, tokens_v, xf_v, part_send, part_own, part_recv,
    gated_v, xcol_v, mix_send, mix_own, mix_recv, xrow_v,
    load_sem, ps_sem, pr_sem, gs_sem, gr_sem, ms_sem, mr_sem, xs_sem, xr_sem, zs_sem, zr_sem, ys_sem, yr_sem,
):
    groups, n, m = sizes
    blocks = memory.shape[0]
    own, heads, dk = memory.shape[1], memory.shape[2], memory.shape[3]
    seqs, feats = tokens.shape
    features = n * feats
    rows, cols = seqs // m, feats // m
    width = heads * dk
    share = width // groups
    grp, dp, tp = lax.axis_index("grp"), lax.axis_index("dp"), lax.axis_index("tp")
    last = blocks - 1

    def mix_slot(b, t):
        return mix_v.at[t] if b == last else mixcol_v.at[b, t]

    def mix_cols(b, to):
        return pl.ds(0, feats) if b == last else pl.ds(pl.multiple_of(to * cols, cols), cols)

    order = [("x", 0, tokens, tokens_v), ("g", 0, gain, gain_v)]
    for b in range(blocks):
        for k, w in enumerate((w_query, w_key, w_value, w_outgate)):
            order.append((f"w{k}", b, w.at[b], w_v.at[b, :, pl.ds(k * width, width)]))
        if b == 0:
            order.append(("gate", 0, gate_w, gate_v))
            order.append(("norm", 0, normalizer, norm_v))
            order.append(("stab", 0, stabilizer, stab_v))
            order.append(("bias", 0, bias_h, bias))
        order.append(("mem", b, memory.at[b], mem_v.at[b]))
        if fast:
            order.append(("mix", b, w_mix.at[b, :, mix_cols(b, tp)], mix_slot(b, tp)))
        else:
            order.append(("mix", b, w_mix.at[b], mix_v.at[b]))
    loads = {}
    for k, (name, b, src, dst) in enumerate(order):
        loads[name, b] = pltpu.make_async_copy(src, dst, load_sem.at[k])
        loads[name, b].start()

    if fast:
        peers = [(od, ot) for ot in range(m) for od in range(n) if (od, ot) != (0, 0)]
    else:
        peers = [(od, 0) for od in range(1, n)] + [(0, ot) for ot in range(1, m)]
    barrier = pltpu.get_barrier_semaphore()

    def at(od, ot, og=0):
        return {"grp": lax.rem(grp + og, groups), "dp": lax.rem(dp + od, n), "tp": lax.rem(tp + ot, m)}

    for od, ot in peers:
        pl.semaphore_signal(barrier, inc=1, device_id=at(od, ot), device_id_type=MESH)
    greeted = len(peers)
    if fast:
        for og in range(1, groups):
            pl.semaphore_signal(barrier, inc=1, device_id=at(0, 0, og), device_id_type=MESH)
        greeted += groups - 1

    sent = []

    def send(src, dst, s_sem, r_sem, where):
        c = pltpu.make_async_remote_copy(
            src_ref=src, dst_ref=dst, send_sem=s_sem, recv_sem=r_sem, device_id=where, device_id_type=MESH
        )
        c.start()
        sent.append(c)
        return c

    def spread(b, offsets):
        part = pl.ds(pl.multiple_of(grp * share, share), share)
        return [
            (o, send(w_mix.at[b, part, mix_cols(b, lax.rem(tp + o, m))], mix_slot(b, tp).at[part],
                     zs_sem.at[b, o - 1], zr_sem.at[b, o - 1], at(0, o)))
            for o in offsets
        ]

    def relay(b, arriving):
        part = pl.ds(pl.multiple_of(grp * share, share), share)
        out = []
        for o, c in arriving:
            c.wait_recv()
            ref = mix_slot(b, lax.rem(tp + m - o, m)).at[part]
            for og in range(1, groups):
                out.append(send(ref, ref, ys_sem.at[b, o - 1, og - 1], yr_sem.at[b, o - 1, og - 1], at(0, 0, og)))
        return out

    diagonal = lax.broadcasted_iota(jnp.int32, (own, own), 0) == lax.broadcasted_iota(jnp.int32, (own, own), 1)
    lane = lax.broadcasted_iota(jnp.int32, (own, 128), 1)
    pending, relayed = {b: [] for b in range(blocks)}, {b: [] for b in range(blocks)}
    loads["x", 0].wait()
    loads["g", 0].wait()
    xf_v[...] = tokens_v[...].astype(F32)
    for b in range(blocks):
        xf = xf_v[...]
        squares = jnp.sum(xf * xf, axis=-1, keepdims=True)
        scaled_in = (xf * gain_v[b:b + 1, :]).astype(BF16)
        if b == 0:
            pl.semaphore_wait(barrier, greeted)
            if fast:
                pending[0] = spread(0, range(1, m))
        for k in range(4):
            loads[f"w{k}", b].wait()
        part = jnp.dot(scaled_in, w_v[b], preferred_element_type=F32)
        for j in range(n):
            piece = part[j * own:(j + 1) * own, :]
            sq = jnp.broadcast_to(squares[j * own:(j + 1) * own, :], (own, 128))
            high = sq.astype(BF16)
            low = (sq - high.astype(F32)).astype(BF16)
            part_send[b, j, :, : 4 * width] = piece.astype(BF16)
            part_send[b, j, :, 4 * width:] = jnp.where(lane < 64, high.astype(F32), low.astype(F32)).astype(BF16)
            part_own[j, :, : 4 * width] = piece
            part_own[j, :, 4 * width:] = jnp.where(lane < 64, sq, 0.0)
        copies = [
            send(part_send.at[b, lax.rem(dp + o, n)], part_recv.at[b, o - 1],
                 ps_sem.at[b, o - 1], pr_sem.at[b, o - 1], at(o, 0))
            for o in range(1, n)
        ]
        if b == 0:
            loads["gate", 0].wait()
            loads["norm", 0].wait()
            loads["stab", 0].wait()
            loads["bias", 0].wait()
        loads["mem", b].wait()
        total = part_own[dp]
        for o, c in enumerate(copies):
            c.wait_recv()
            total = total + part_recv[b, o].astype(F32)
        own_sq = total[:, 4 * width:4 * width + 1] + total[:, 4 * width + 64:4 * width + 65]
        scale = lax.rsqrt(own_sq / features + EPS)
        projs = (scale * total[:, : 4 * width]).astype(BF16)
        mine = gated_v.at[b, tp if fast else 0, dp]
        updates = []
        for h in range(heads):
            query, key, value, outgate = (
                projs[:, k * width + h * dk:k * width + (h + 1) * dk].astype(F32) for k in range(4)
            )
            gate = gate_v[b, h].astype(F32)

            def pre(g):
                terms = (
                    query * gate[g:g + 1, :dk] + key * gate[g:g + 1, dk:2 * dk] + value * gate[g:g + 1, 2 * dk:]
                )
                return jnp.sum(terms, axis=-1, keepdims=True)

            log_input = pre(0)
            z = pre(1) + bias[h, b]
            log_forget = jnp.minimum(z, 0.0) - jnp.log1p(jnp.exp(-jnp.abs(z)))
            stab = jnp.sum(jnp.where(diagonal, stab_v[b, h:h + 1, :], 0.0), axis=1, keepdims=True)
            new_stab = jnp.maximum(log_forget + stab, log_input)
            keep = jnp.exp(log_forget + stab - new_stab)
            admit = jnp.exp(log_input - new_stab)
            ak = admit * (key * dk ** (-0.5))
            new_norm = keep * norm_v[b, :, h * dk:(h + 1) * dk] + ak
            query_t = query.T
            held = jnp.concatenate(
                [jnp.sum(query_t[:, s:s + 1] * mem_v[b, s, h], axis=0, keepdims=True) for s in range(own)], axis=0
            )
            numer = keep * held + jnp.sum(query * ak, axis=-1, keepdims=True) * value
            denom = jnp.maximum(jnp.abs(jnp.sum(query * new_norm, axis=-1, keepdims=True)), 1.0)
            mine[:, h * dk:(h + 1) * dk] = (numer / denom * jax.nn.sigmoid(outgate)).astype(BF16)
            updates.append((keep, ak, value, new_stab, new_norm))
        to = [(od, ot) for ot in reversed(range(m if fast else 1)) for od in range(n) if (od, ot) != (0, 0)]
        copies = [
            send(mine, mine, gs_sem.at[b, ot * n + od], gr_sem.at[b, ot * n + od], at(od, ot)) for od, ot in to
        ]
        if fast:
            if b + 1 == last:
                early = spread(last, range(1, m, 2))
            relayed[b] += relay(b, pending[b])
        for h, (keep, ak, value, new_stab, new_norm) in enumerate(updates):
            stab_out[b, h:h + 1, :] = jnp.sum(jnp.where(diagonal, new_stab, 0.0), axis=0, keepdims=True)
            norm_out[b, :, h * dk:(h + 1) * dk] = new_norm
            ak_t = ak.T
            kept = jnp.broadcast_to(keep, (own, dk))
            for s in range(own):
                memory_out[b, s, h] = kept[s:s + 1, :] * mem_v[b, s, h] + ak_t[:, s:s + 1] * value[s:s + 1, :]
        loads["mix", b].wait()
        for c in copies + relayed[b]:
            c.wait_recv()
        if fast:
            every = jnp.concatenate([gated_v[b, t].reshape(n * own, width) for t in range(m)], axis=1)
        if fast and b == last:
            mixed = jnp.dot(every, mix_v[...].reshape(m * width, feats), preferred_element_type=F32)
            x_out[...] = (xf_v[...] + mixed).astype(BF16)
        elif fast:
            mixed = jnp.dot(every, mixcol_v[b].reshape(m * width, cols), preferred_element_type=F32)
            own_cols = xf_v[:, pl.ds(pl.multiple_of(tp * cols, cols), cols)]
            xcol_v[b, tp] = (own_cols + mixed).astype(BF16)
            ref = xcol_v.at[b, tp]
            copies = [send(ref, ref, xs_sem.at[b, o - 1], xr_sem.at[b, o - 1], at(0, o)) for o in range(1, m)]
            if b + 1 == last:
                pending[last] = spread(last, range(2, m, 2))
            else:
                pending[b + 1] = spread(b + 1, range(1, m))
            for c in copies:
                c.wait_recv()
            if b + 1 == last:
                relayed[last] += relay(last, early)
            for j in range(m):
                xf_v[:, j * cols:(j + 1) * cols] = xcol_v[b, j].astype(F32)
        else:
            every = gated_v[b, 0].reshape(n * own, width)
            mixed = jnp.dot(every, mix_v[b], preferred_element_type=F32)
            for j in range(m):
                piece = mixed[j * rows:(j + 1) * rows, :]
                mix_send[b, j] = piece.astype(BF16)
                mix_own[j] = piece
                xrow_v[j] = xf_v[j * rows:(j + 1) * rows, :].astype(BF16)
            copies = [
                send(mix_send.at[b, lax.rem(tp + o, m)], mix_recv.at[b, o - 1],
                     ms_sem.at[b, o - 1], mr_sem.at[b, o - 1], at(0, o))
                for o in range(1, m)
            ]
            total = mix_own[tp]
            for o, c in enumerate(copies):
                c.wait_recv()
                total = total + mix_recv[b, o].astype(F32)
            xcol_v[b, tp] = (xrow_v[tp].astype(F32) + total).astype(BF16)
            ref = xcol_v.at[b, tp]
            copies = [send(ref, ref, xs_sem.at[b, o - 1], xr_sem.at[b, o - 1], at(0, o)) for o in range(1, m)]
            for c in copies:
                c.wait_recv()
            for j in range(m):
                xf_v[j * rows:(j + 1) * rows, :] = xcol_v[b, j].astype(F32)
            if b == last:
                x_out[...] = xf_v[...].astype(BF16)
    for c in sent:
        c.wait_send()


def store_kernel(*refs):
    count = (len(refs) - 1) // 2
    sources, results, sem = refs[:count], refs[count:2 * count], refs[-1]
    copies = [pltpu.make_async_copy(a, z, sem.at[k]) for k, (a, z) in enumerate(zip(sources, results))]
    for c in copies:
        c.start()
    for c in copies:
        c.wait()


def shards(sizes, tokens, norm_gain, w_query, w_key, w_value, w_outgate, gate_weight, forget_bias, w_mix, memory, normalizer, stabilizer):
    groups, n, m = sizes
    seqs, feats = tokens.shape
    blocks, own, heads, dk, _ = memory.shape
    width = heads * dk
    rows, cols = seqs // m, feats // m
    wide = 4 * width + 128
    fast = cols % 128 == 0 and width % (16 * groups) == 0 and blocks > 1
    hbm = pl.BlockSpec(memory_space=pltpu.HBM)
    vmem = pl.BlockSpec(memory_space=pltpu.VMEM)
    dma = pltpu.SemaphoreType.DMA
    nd, nt, ng = max(n - 1, 1), max(m - 1, 1), max(groups - 1, 1)
    slow_rows = (1, 8, 128) if fast else (m, rows, feats)
    results = (
        ((seqs, feats), BF16),
        (memory.shape, F32),
        ((blocks, own, width), F32),
        ((blocks, heads, own), F32),
    )
    held = pl.pallas_call(
        functools.partial(step_kernel, sizes, fast),
        out_shape=tuple(pltpu.VMEM(shape, kind) for shape, kind in results),
        in_specs=[hbm] * 12,
        out_specs=(vmem,) * 4,
        scratch_shapes=[
            pltpu.VMEM(norm_gain.shape, F32),
            pltpu.VMEM((blocks, feats, 4 * width), BF16),
            pltpu.VMEM((blocks, heads, 2, 3 * dk), BF16),
            pltpu.VMEM((m, width, feats) if fast else w_mix.shape, BF16),
            pltpu.VMEM((blocks - 1, m, width, cols) if fast else (1, 1, 16, 128), BF16),
            pltpu.VMEM(memory.shape, F32),
            pltpu.VMEM((blocks, own, width), F32),
            pltpu.VMEM((blocks, heads, own), F32),
            pltpu.SMEM((heads, blocks), F32),
            pltpu.VMEM((seqs, feats), BF16),
            pltpu.VMEM((seqs, feats), F32),
            pltpu.VMEM((blocks, n, own, wide), BF16),
            pltpu.VMEM((n, own, wide), F32),
            pltpu.VMEM((blocks, nd, own, wide), BF16),
            pltpu.VMEM((blocks, m if fast else 1, n, own, width), BF16),
            pltpu.VMEM((blocks, m, seqs, cols) if fast else (blocks, m, rows, feats), BF16),
            pltpu.VMEM((blocks,) + slow_rows, BF16),
            pltpu.VMEM(slow_rows, F32),
            pltpu.VMEM((blocks, nt) + slow_rows[1:], BF16),
            pltpu.VMEM(slow_rows, BF16),
            dma((6 + 6 * blocks,)),
            dma((blocks, nd)), dma((blocks, nd)), dma((blocks, n * m)), dma((blocks, n * m)),
            dma((blocks, nt)), dma((blocks, nt)), dma((blocks, nt)), dma((blocks, nt)),
            dma((blocks, nt)), dma((blocks, nt)), dma((blocks, nt, ng)), dma((blocks, nt, ng)),
        ],
        compiler_params=pltpu.CompilerParams(collective_id=0, has_side_effects=True, vmem_limit_bytes=32 << 20),
    )(
        *(
            pltpu.with_memory_space_constraint(t, pltpu.HBM)
            for t in (
                tokens, norm_gain, w_query, w_key, w_value, w_outgate,
                jnp.swapaxes(gate_weight, 2, 3), w_mix, memory, normalizer.reshape(blocks, own, width),
                jnp.swapaxes(stabilizer, 1, 2), forget_bias.T,
            )
        ),
    )
    x, new_memory, norm, stab = pl.pallas_call(
        store_kernel,
        out_shape=tuple(jax.ShapeDtypeStruct(shape, kind) for shape, kind in results),
        in_specs=[vmem] * 4,
        out_specs=(pl.BlockSpec(memory_space=pl.ANY),) * 4,
        scratch_shapes=[dma((4,))],
    )(*(pltpu.with_memory_space_constraint(t, pltpu.VMEM) for t in held))
    return x, new_memory, norm.reshape(normalizer.shape), jnp.swapaxes(stab, 1, 2)


def solution(mesh):
    in_specs = (
        P("grp", "dp"),
        P(None, "dp"),
        P(None, "dp", "tp"),
        P(None, "dp", "tp"),
        P(None, "dp", "tp"),
        P(None, "dp", "tp"),
        P(None, "tp", None, None),
        P(None, "tp"),
        P(None, "tp", "dp"),
        P(None, ("grp", "dp"), "tp", None, None),
        P(None, ("grp", "dp"), "tp", None),
        P(None, ("grp", "dp"), "tp"),
    )
    out_specs = (
        P("grp", "dp"),
        P(None, ("grp", "dp"), "tp", None, None),
        P(None, ("grp", "dp"), "tp", None),
        P(None, ("grp", "dp"), "tp"),
    )
    body = functools.partial(shards, (mesh.shape["grp"], mesh.shape["dp"], mesh.shape["tp"]))
    return jax.shard_map(body, mesh=mesh, in_specs=in_specs, out_specs=out_specs, check_vma=False)
```

```python
import functools

import jax
import jax.numpy as jnp
from jax import lax
from jax.experimental import pallas as pl
from jax.experimental.pallas import tpu as pltpu
from jax.sharding import PartitionSpec as P

EPS = 1e-06
F32 = jnp.float32
BF16 = jnp.bfloat16
MESH = pl.DeviceIdType.MESH


def step_kernel(
    sizes, fast,
    tokens, gain, w_query, w_key, w_value, w_outgate, gate_w, w_mix, memory, normalizer, stabilizer, bias_h,
    x_out, memory_out, norm_out, stab_out,
    gain_v, w_v, gate_v, mix_v, mixcol_v, mem_v, norm_v, stab_v, bias, tokens_v, xf_v, part_send, part_own, part_recv,
    gated_v, xcol_v, mix_send, mix_own, mix_recv, xrow_v,
    load_sem, ps_sem, pr_sem, gs_sem, gr_sem, ms_sem, mr_sem, xs_sem, xr_sem, zs_sem, zr_sem, ys_sem, yr_sem,
):
    groups, n, m = sizes
    blocks = memory.shape[0]
    own, heads, dk = memory.shape[1], memory.shape[2], memory.shape[3]
    seqs, feats = tokens.shape
    features = n * feats
    rows, cols = seqs // m, feats // m
    width = heads * dk
    share = width // groups
    grp, dp, tp = lax.axis_index("grp"), lax.axis_index("dp"), lax.axis_index("tp")
    last = blocks - 1

    def mix_slot(b, t):
        return mixcol_v.at[b, t]

    def mix_cols(b, to):
        return pl.ds(pl.multiple_of(to * cols, cols), cols)

    order = [("x", 0, tokens, tokens_v), ("g", 0, gain, gain_v)]
    for b in range(blocks):
        for k, w in enumerate((w_query, w_key, w_value, w_outgate)):
            order.append((f"w{k}", b, w.at[b], w_v.at[b, :, pl.ds(k * width, width)]))
        if b == 0:
            order.append(("gate", 0, gate_w, gate_v))
            order.append(("norm", 0, normalizer, norm_v))
            order.append(("stab", 0, stabilizer, stab_v))
            order.append(("bias", 0, bias_h, bias))
        order.append(("mem", b, memory.at[b], mem_v.at[b]))
        if fast:
            order.append(("mix", b, w_mix.at[b, :, mix_cols(b, tp)], mix_slot(b, tp)))
        else:
            order.append(("mix", b, w_mix.at[b], mix_v.at[b]))
    loads = {}
    for k, (name, b, src, dst) in enumerate(order):
        loads[name, b] = pltpu.make_async_copy(src, dst, load_sem.at[k])
        loads[name, b].start()

    if fast:
        peers = [(od, ot) for ot in range(m) for od in range(n) if (od, ot) != (0, 0)]
    else:
        peers = [(od, 0) for od in range(1, n)] + [(0, ot) for ot in range(1, m)]
    barrier = pltpu.get_barrier_semaphore()

    def at(od, ot, og=0):
        return {"grp": lax.rem(grp + og, groups), "dp": lax.rem(dp + od, n), "tp": lax.rem(tp + ot, m)}

    for od, ot in peers:
        pl.semaphore_signal(barrier, inc=1, device_id=at(od, ot), device_id_type=MESH)
    greeted = len(peers)
    if fast:
        for og in range(1, groups):
            pl.semaphore_signal(barrier, inc=1, device_id=at(0, 0, og), device_id_type=MESH)
        greeted += groups - 1

    sent = []

    def send(src, dst, s_sem, r_sem, where):
        c = pltpu.make_async_remote_copy(
            src_ref=src, dst_ref=dst, send_sem=s_sem, recv_sem=r_sem, device_id=where, device_id_type=MESH
        )
        c.start()
        sent.append(c)
        return c

    def spread(b, offsets):
        part = pl.ds(pl.multiple_of(grp * share, share), share)
        return [
            (o, send(w_mix.at[b, part, mix_cols(b, lax.rem(tp + o, m))], mix_slot(b, tp).at[part],
                     zs_sem.at[b, o - 1], zr_sem.at[b, o - 1], at(0, o)))
            for o in offsets
        ]

    def relay(b, arriving):
        part = pl.ds(pl.multiple_of(grp * share, share), share)
        out = []
        for o, c in arriving:
            c.wait_recv()
            ref = mix_slot(b, lax.rem(tp + m - o, m)).at[part]
            for og in range(1, groups):
                out.append(send(ref, ref, ys_sem.at[b, o - 1, og - 1], yr_sem.at[b, o - 1, og - 1], at(0, 0, og)))
        return out

    diagonal = lax.broadcasted_iota(jnp.int32, (own, own), 0) == lax.broadcasted_iota(jnp.int32, (own, own), 1)
    lane = lax.broadcasted_iota(jnp.int32, (own, 128), 1)
    pending, relayed = {b: [] for b in range(blocks)}, {b: [] for b in range(blocks)}
    loads["x", 0].wait()
    loads["g", 0].wait()
    xf_v[...] = tokens_v[...].astype(F32)
    for b in range(blocks):
        xf = xf_v[...]
        squares = jnp.sum(xf * xf, axis=-1, keepdims=True)
        scaled_in = (xf * gain_v[b:b + 1, :]).astype(BF16)
        if b == 0:
            pl.semaphore_wait(barrier, greeted)
            if fast:
                pending[0] = spread(0, range(1, m))
        for k in range(4):
            loads[f"w{k}", b].wait()
        part = jnp.dot(scaled_in, w_v[b], preferred_element_type=F32)
        for j in range(n):
            piece = part[j * own:(j + 1) * own, :]
            sq = jnp.broadcast_to(squares[j * own:(j + 1) * own, :], (own, 128))
            high = sq.astype(BF16)
            low = (sq - high.astype(F32)).astype(BF16)
            part_send[b, j, :, : 4 * width] = piece.astype(BF16)
            part_send[b, j, :, 4 * width:] = jnp.where(lane < 64, high.astype(F32), low.astype(F32)).astype(BF16)
            part_own[j, :, : 4 * width] = piece
            part_own[j, :, 4 * width:] = jnp.where(lane < 64, sq, 0.0)
        copies = [
            send(part_send.at[b, lax.rem(dp + o, n)], part_recv.at[b, o - 1],
                 ps_sem.at[b, o - 1], pr_sem.at[b, o - 1], at(o, 0))
            for o in range(1, n)
        ]
        if b == 0:
            loads["gate", 0].wait()
            loads["norm", 0].wait()
            loads["stab", 0].wait()
            loads["bias", 0].wait()
        loads["mem", b].wait()
        total = part_own[dp]
        for o, c in enumerate(copies):
            c.wait_recv()
            total = total + part_recv[b, o].astype(F32)
        own_sq = total[:, 4 * width:4 * width + 1] + total[:, 4 * width + 64:4 * width + 65]
        scale = lax.rsqrt(own_sq / features + EPS)
        projs = (scale * total[:, : 4 * width]).astype(BF16)
        mine = gated_v.at[b, tp if fast else 0, dp]
        updates = []
        for h in range(heads):
            query, key, value, outgate = (
                projs[:, k * width + h * dk:k * width + (h + 1) * dk].astype(F32) for k in range(4)
            )
            gate = gate_v[b, h].astype(F32)

            def pre(g):
                terms = (
                    query * gate[g:g + 1, :dk] + key * gate[g:g + 1, dk:2 * dk] + value * gate[g:g + 1, 2 * dk:]
                )
                return jnp.sum(terms, axis=-1, keepdims=True)

            log_input = pre(0)
            z = pre(1) + bias[h, b]
            log_forget = jnp.minimum(z, 0.0) - jnp.log1p(jnp.exp(-jnp.abs(z)))
            stab = jnp.sum(jnp.where(diagonal, stab_v[b, h:h + 1, :], 0.0), axis=1, keepdims=True)
            new_stab = jnp.maximum(log_forget + stab, log_input)
            keep = jnp.exp(log_forget + stab - new_stab)
            admit = jnp.exp(log_input - new_stab)
            ak = admit * (key * dk ** (-0.5))
            new_norm = keep * norm_v[b, :, h * dk:(h + 1) * dk] + ak
            query_t = query.T
            held = jnp.concatenate(
                [jnp.sum(query_t[:, s:s + 1] * mem_v[b, s, h], axis=0, keepdims=True) for s in range(own)], axis=0
            )
            numer = keep * held + jnp.sum(query * ak, axis=-1, keepdims=True) * value
            denom = jnp.maximum(jnp.abs(jnp.sum(query * new_norm, axis=-1, keepdims=True)), 1.0)
            mine[:, h * dk:(h + 1) * dk] = (numer / denom * jax.nn.sigmoid(outgate)).astype(BF16)
            updates.append((keep, ak, value, new_stab, new_norm))
        to = [(od, ot) for ot in reversed(range(m if fast else 1)) for od in range(n) if (od, ot) != (0, 0)]
        copies = [
            send(mine, mine, gs_sem.at[b, ot * n + od], gr_sem.at[b, ot * n + od], at(od, ot)) for od, ot in to
        ]
        if fast:
            relayed[b] += relay(b, pending[b])
            if b < last:
                pending[b + 1] = spread(b + 1, range(1, m))
        for h, (keep, ak, value, new_stab, new_norm) in enumerate(updates):
            stab_out[b, h:h + 1, :] = jnp.sum(jnp.where(diagonal, new_stab, 0.0), axis=0, keepdims=True)
            norm_out[b, :, h * dk:(h + 1) * dk] = new_norm
            ak_t = ak.T
            kept = jnp.broadcast_to(keep, (own, dk))
            for s in range(own):
                memory_out[b, s, h] = kept[s:s + 1, :] * mem_v[b, s, h] + ak_t[:, s:s + 1] * value[s:s + 1, :]
        loads["mix", b].wait()
        for c in copies + relayed[b]:
            c.wait_recv()
        if fast:
            every = jnp.concatenate([gated_v[b, t].reshape(n * own, width) for t in range(m)], axis=1)
        if fast:
            mixed = jnp.dot(every, mixcol_v[b].reshape(m * width, cols), preferred_element_type=F32)
            own_cols = xf_v[:, pl.ds(pl.multiple_of(tp * cols, cols), cols)]
            xcol_v[b, tp] = (own_cols + mixed).astype(BF16)
            ref = xcol_v.at[b, tp]
            copies = [send(ref, ref, xs_sem.at[b, o - 1], xr_sem.at[b, o - 1], at(0, o)) for o in range(1, m)]
            for c in copies:
                c.wait_recv()
            for j in range(m):
                if b == last:
                    x_out[:, j * cols:(j + 1) * cols] = xcol_v[b, j]
                else:
                    xf_v[:, j * cols:(j + 1) * cols] = xcol_v[b, j].astype(F32)
        else:
            every = gated_v[b, 0].reshape(n * own, width)
            mixed = jnp.dot(every, mix_v[b], preferred_element_type=F32)
            for j in range(m):
                piece = mixed[j * rows:(j + 1) * rows, :]
                mix_send[b, j] = piece.astype(BF16)
                mix_own[j] = piece
                xrow_v[j] = xf_v[j * rows:(j + 1) * rows, :].astype(BF16)
            copies = [
                send(mix_send.at[b, lax.rem(tp + o, m)], mix_recv.at[b, o - 1],
                     ms_sem.at[b, o - 1], mr_sem.at[b, o - 1], at(0, o))
                for o in range(1, m)
            ]
            total = mix_own[tp]
            for o, c in enumerate(copies):
                c.wait_recv()
                total = total + mix_recv[b, o].astype(F32)
            xcol_v[b, tp] = (xrow_v[tp].astype(F32) + total).astype(BF16)
            ref = xcol_v.at[b, tp]
            copies = [send(ref, ref, xs_sem.at[b, o - 1], xr_sem.at[b, o - 1], at(0, o)) for o in range(1, m)]
            for c in copies:
                c.wait_recv()
            for j in range(m):
                xf_v[j * rows:(j + 1) * rows, :] = xcol_v[b, j].astype(F32)
            if b == last:
                x_out[...] = xf_v[...].astype(BF16)
    for c in sent:
        c.wait_send()


def store_kernel(*refs):
    count = (len(refs) - 1) // 2
    sources, results, sem = refs[:count], refs[count:2 * count], refs[-1]
    copies = [pltpu.make_async_copy(a, z, sem.at[k]) for k, (a, z) in enumerate(zip(sources, results))]
    for c in copies:
        c.start()
    for c in copies:
        c.wait()


def shards(sizes, tokens, norm_gain, w_query, w_key, w_value, w_outgate, gate_weight, forget_bias, w_mix, memory, normalizer, stabilizer):
    groups, n, m = sizes
    seqs, feats = tokens.shape
    blocks, own, heads, dk, _ = memory.shape
    width = heads * dk
    rows, cols = seqs // m, feats // m
    wide = 4 * width + 128
    fast = cols % 128 == 0 and width % (16 * groups) == 0
    hbm = pl.BlockSpec(memory_space=pltpu.HBM)
    vmem = pl.BlockSpec(memory_space=pltpu.VMEM)
    dma = pltpu.SemaphoreType.DMA
    nd, nt, ng = max(n - 1, 1), max(m - 1, 1), max(groups - 1, 1)
    slow_rows = (1, 8, 128) if fast else (m, rows, feats)
    results = (
        ((seqs, feats), BF16),
        (memory.shape, F32),
        ((blocks, own, width), F32),
        ((blocks, heads, own), F32),
    )
    held = pl.pallas_call(
        functools.partial(step_kernel, sizes, fast),
        out_shape=tuple(pltpu.VMEM(shape, kind) for shape, kind in results),
        in_specs=[hbm] * 12,
        out_specs=(vmem,) * 4,
        scratch_shapes=[
            pltpu.VMEM(norm_gain.shape, F32),
            pltpu.VMEM((blocks, feats, 4 * width), BF16),
            pltpu.VMEM((blocks, heads, 2, 3 * dk), BF16),
            pltpu.VMEM((1, 16, 128) if fast else w_mix.shape, BF16),
            pltpu.VMEM((blocks, m, width, cols) if fast else (1, 1, 16, 128), BF16),
            pltpu.VMEM(memory.shape, F32),
            pltpu.VMEM((blocks, own, width), F32),
            pltpu.VMEM((blocks, heads, own), F32),
            pltpu.SMEM((heads, blocks), F32),
            pltpu.VMEM((seqs, feats), BF16),
            pltpu.VMEM((seqs, feats), F32),
            pltpu.VMEM((blocks, n, own, wide), BF16),
            pltpu.VMEM((n, own, wide), F32),
            pltpu.VMEM((blocks, nd, own, wide), BF16),
            pltpu.VMEM((blocks, m if fast else 1, n, own, width), BF16),
            pltpu.VMEM((blocks, m, seqs, cols) if fast else (blocks, m, rows, feats), BF16),
            pltpu.VMEM((blocks,) + slow_rows, BF16),
            pltpu.VMEM(slow_rows, F32),
            pltpu.VMEM((blocks, nt) + slow_rows[1:], BF16),
            pltpu.VMEM(slow_rows, BF16),
            dma((6 + 6 * blocks,)),
            dma((blocks, nd)), dma((blocks, nd)), dma((blocks, n * m)), dma((blocks, n * m)),
            dma((blocks, nt)), dma((blocks, nt)), dma((blocks, nt)), dma((blocks, nt)),
            dma((blocks, nt)), dma((blocks, nt)), dma((blocks, nt, ng)), dma((blocks, nt, ng)),
        ],
        compiler_params=pltpu.CompilerParams(collective_id=0, has_side_effects=True, vmem_limit_bytes=32 << 20),
    )(
        *(
            pltpu.with_memory_space_constraint(t, pltpu.HBM)
            for t in (
                tokens, norm_gain, w_query, w_key, w_value, w_outgate,
                jnp.swapaxes(gate_weight, 2, 3), w_mix, memory, normalizer.reshape(blocks, own, width),
                jnp.swapaxes(stabilizer, 1, 2), forget_bias.T,
            )
        ),
    )
    x, new_memory, norm, stab = pl.pallas_call(
        store_kernel,
        out_shape=tuple(jax.ShapeDtypeStruct(shape, kind) for shape, kind in results),
        in_specs=[vmem] * 4,
        out_specs=(pl.BlockSpec(memory_space=pl.ANY),) * 4,
        scratch_shapes=[dma((4,))],
    )(*(pltpu.with_memory_space_constraint(t, pltpu.VMEM) for t in held))
    return x, new_memory, norm.reshape(normalizer.shape), jnp.swapaxes(stab, 1, 2)


def solution(mesh):
    in_specs = (
        P("grp", "dp"),
        P(None, "dp"),
        P(None, "dp", "tp"),
        P(None, "dp", "tp"),
        P(None, "dp", "tp"),
        P(None, "dp", "tp"),
        P(None, "tp", None, None),
        P(None, "tp"),
        P(None, "tp", "dp"),
        P(None, ("grp", "dp"), "tp", None, None),
        P(None, ("grp", "dp"), "tp", None),
        P(None, ("grp", "dp"), "tp"),
    )
    out_specs = (
        P("grp", "dp"),
        P(None, ("grp", "dp"), "tp", None, None),
        P(None, ("grp", "dp"), "tp", None),
        P(None, ("grp", "dp"), "tp"),
    )
    body = functools.partial(shards, (mesh.shape["grp"], mesh.shape["dp"], mesh.shape["tp"]))
    return jax.shard_map(body, mesh=mesh, in_specs=in_specs, out_specs=out_specs, check_vma=False)
```

```python
import functools

import jax
import jax.numpy as jnp
from jax import lax
from jax.experimental import pallas as pl
from jax.experimental.pallas import tpu as pltpu
from jax.sharding import PartitionSpec as P

EPS = 1e-06
F32 = jnp.float32
BF16 = jnp.bfloat16
MESH = pl.DeviceIdType.MESH


def step_kernel(
    sizes, fast,
    tokens, gain, w_query, w_key, w_value, w_outgate, gate_w, w_mix, memory, normalizer, stabilizer, bias_h,
    x_out, memory_out, norm_out, stab_out,
    gain_v, w_v, gate_v, mix_v, mixcol_v, mem_v, norm_v, stab_v, bias, tokens_v, xf_v, part_send, part_own, part_recv,
    gated_v, xcol_v, mix_send, mix_own, mix_recv, xrow_v,
    load_sem, ps_sem, pr_sem, gs_sem, gr_sem, ms_sem, mr_sem, xs_sem, xr_sem, zs_sem, zr_sem, ys_sem, yr_sem,
):
    groups, n, m = sizes
    blocks = memory.shape[0]
    own, heads, dk = memory.shape[1], memory.shape[2], memory.shape[3]
    seqs, feats = tokens.shape
    features = n * feats
    rows, cols = seqs // m, feats // m
    width = heads * dk
    share = width // groups
    grp, dp, tp = lax.axis_index("grp"), lax.axis_index("dp"), lax.axis_index("tp")
    last = blocks - 1

    def mix_slot(b, t):
        return mixcol_v.at[b, t]

    def mix_cols(b, to):
        return pl.ds(pl.multiple_of(to * cols, cols), cols)

    order = [("x", 0, tokens, tokens_v), ("g", 0, gain, gain_v)]
    for b in range(blocks):
        for k, w in enumerate((w_query, w_key, w_value, w_outgate)):
            order.append((f"w{k}", b, w.at[b], w_v.at[b, :, pl.ds(k * width, width)]))
        if b == 0:
            order.append(("gate", 0, gate_w, gate_v))
            order.append(("norm", 0, normalizer, norm_v))
            order.append(("stab", 0, stabilizer, stab_v))
            order.append(("bias", 0, bias_h, bias))
        order.append(("mem", b, memory.at[b], mem_v.at[b]))
        if fast:
            order.append(("mix", b, w_mix.at[b, :, mix_cols(b, tp)], mix_slot(b, tp)))
        else:
            order.append(("mix", b, w_mix.at[b], mix_v.at[b]))
    loads = {}
    for k, (name, b, src, dst) in enumerate(order):
        loads[name, b] = pltpu.make_async_copy(src, dst, load_sem.at[k])
        loads[name, b].start()

    if fast:
        peers = [(od, ot) for ot in range(m) for od in range(n) if (od, ot) != (0, 0)]
    else:
        peers = [(od, 0) for od in range(1, n)] + [(0, ot) for ot in range(1, m)]
    barrier = pltpu.get_barrier_semaphore()

    def at(od, ot, og=0):
        return {"grp": lax.rem(grp + og, groups), "dp": lax.rem(dp + od, n), "tp": lax.rem(tp + ot, m)}

    for od, ot in peers:
        pl.semaphore_signal(barrier, inc=1, device_id=at(od, ot), device_id_type=MESH)
    greeted = len(peers)
    if fast:
        for og in range(1, groups):
            pl.semaphore_signal(barrier, inc=1, device_id=at(0, 0, og), device_id_type=MESH)
        greeted += groups - 1

    sent = []

    def send(src, dst, s_sem, r_sem, where):
        c = pltpu.make_async_remote_copy(
            src_ref=src, dst_ref=dst, send_sem=s_sem, recv_sem=r_sem, device_id=where, device_id_type=MESH
        )
        c.start()
        sent.append(c)
        return c

    def spread(b, offsets):
        part = pl.ds(pl.multiple_of(grp * share, share), share)
        return [
            (o, send(w_mix.at[b, part, mix_cols(b, lax.rem(tp + o, m))], mix_slot(b, tp).at[part],
                     zs_sem.at[b, o - 1], zr_sem.at[b, o - 1], at(0, o)))
            for o in offsets
        ]

    def relay(b, arriving):
        part = pl.ds(pl.multiple_of(grp * share, share), share)
        out = []
        for o, c in arriving:
            c.wait_recv()
            ref = mix_slot(b, lax.rem(tp + m - o, m)).at[part]
            for og in range(1, groups):
                out.append(send(ref, ref, ys_sem.at[b, o - 1, og - 1], yr_sem.at[b, o - 1, og - 1], at(0, 0, og)))
        return out

    diagonal = lax.broadcasted_iota(jnp.int32, (own, own), 0) == lax.broadcasted_iota(jnp.int32, (own, own), 1)
    lane = lax.broadcasted_iota(jnp.int32, (own, 128), 1)
    pending, relayed = {b: [] for b in range(blocks)}, {b: [] for b in range(blocks)}
    loads["x", 0].wait()
    loads["g", 0].wait()
    xf_v[...] = tokens_v[...].astype(F32)
    for b in range(blocks):
        by_piece = fast and b > 0
        if not by_piece:
            xf = xf_v[...]
            squares = jnp.sum(xf * xf, axis=-1, keepdims=True)
            scaled_in = (xf * gain_v[b:b + 1, :]).astype(BF16)
        if b == 0:
            pl.semaphore_wait(barrier, greeted)
            if fast:
                pending[0] = spread(0, range(1, m))
        for k in range(4):
            loads[f"w{k}", b].wait()
        if by_piece:
            for o in range(m):
                if o:
                    arriving[o - 1].wait_recv()
                frm = lax.rem(tp + m - o, m)
                where = pl.ds(pl.multiple_of(frm * cols, cols), cols)
                xf = xcol_v[b - 1, frm].astype(F32)
                square = jnp.sum(xf * xf, axis=-1, keepdims=True)
                scaled_in = (xf * gain_v[b:b + 1, where]).astype(BF16)
                term = jnp.dot(scaled_in, w_v[b, where, :], preferred_element_type=F32)
                part, squares = (part + term, squares + square) if o else (term, square)
        else:
            part = jnp.dot(scaled_in, w_v[b], preferred_element_type=F32)
        for j in range(n):
            piece = part[j * own:(j + 1) * own, :]
            sq = jnp.broadcast_to(squares[j * own:(j + 1) * own, :], (own, 128))
            high = sq.astype(BF16)
            low = (sq - high.astype(F32)).astype(BF16)
            part_send[b, j, :, : 4 * width] = piece.astype(BF16)
            part_send[b, j, :, 4 * width:] = jnp.where(lane < 64, high.astype(F32), low.astype(F32)).astype(BF16)
            part_own[j, :, : 4 * width] = piece
            part_own[j, :, 4 * width:] = jnp.where(lane < 64, sq, 0.0)
        copies = [
            send(part_send.at[b, lax.rem(dp + o, n)], part_recv.at[b, o - 1],
                 ps_sem.at[b, o - 1], pr_sem.at[b, o - 1], at(o, 0))
            for o in range(1, n)
        ]
        if b == 0:
            loads["gate", 0].wait()
            loads["norm", 0].wait()
            loads["stab", 0].wait()
            loads["bias", 0].wait()
        loads["mem", b].wait()
        total = part_own[dp]
        for o, c in enumerate(copies):
            c.wait_recv()
            total = total + part_recv[b, o].astype(F32)
        own_sq = total[:, 4 * width:4 * width + 1] + total[:, 4 * width + 64:4 * width + 65]
        scale = lax.rsqrt(own_sq / features + EPS)
        projs = (scale * total[:, : 4 * width]).astype(BF16)
        mine = gated_v.at[b, tp if fast else 0, dp]
        updates = []
        for h in range(heads):
            query, key, value, outgate = (
                projs[:, k * width + h * dk:k * width + (h + 1) * dk].astype(F32) for k in range(4)
            )
            gate = gate_v[b, h].astype(F32)

            def pre(g):
                terms = (
                    query * gate[g:g + 1, :dk] + key * gate[g:g + 1, dk:2 * dk] + value * gate[g:g + 1, 2 * dk:]
                )
                return jnp.sum(terms, axis=-1, keepdims=True)

            log_input = pre(0)
            z = pre(1) + bias[h, b]
            log_forget = jnp.minimum(z, 0.0) - jnp.log1p(jnp.exp(-jnp.abs(z)))
            stab = jnp.sum(jnp.where(diagonal, stab_v[b, h:h + 1, :], 0.0), axis=1, keepdims=True)
            new_stab = jnp.maximum(log_forget + stab, log_input)
            keep = jnp.exp(log_forget + stab - new_stab)
            admit = jnp.exp(log_input - new_stab)
            ak = admit * (key * dk ** (-0.5))
            new_norm = keep * norm_v[b, :, h * dk:(h + 1) * dk] + ak
            query_t = query.T
            held = jnp.concatenate(
                [jnp.sum(query_t[:, s:s + 1] * mem_v[b, s, h], axis=0, keepdims=True) for s in range(own)], axis=0
            )
            numer = keep * held + jnp.sum(query * ak, axis=-1, keepdims=True) * value
            denom = jnp.maximum(jnp.abs(jnp.sum(query * new_norm, axis=-1, keepdims=True)), 1.0)
            mine[:, h * dk:(h + 1) * dk] = (numer / denom * jax.nn.sigmoid(outgate)).astype(BF16)
            updates.append((keep, ak, value, new_stab, new_norm))
        to = [(od, ot) for ot in reversed(range(m if fast else 1)) for od in range(n) if (od, ot) != (0, 0)]
        copies = [
            send(mine, mine, gs_sem.at[b, ot * n + od], gr_sem.at[b, ot * n + od], at(od, ot)) for od, ot in to
        ]
        if fast:
            relayed[b] += relay(b, pending[b])
            if b < last:
                pending[b + 1] = spread(b + 1, range(1, m))
        for h, (keep, ak, value, new_stab, new_norm) in enumerate(updates):
            stab_out[b, h:h + 1, :] = jnp.sum(jnp.where(diagonal, new_stab, 0.0), axis=0, keepdims=True)
            norm_out[b, :, h * dk:(h + 1) * dk] = new_norm
            ak_t = ak.T
            kept = jnp.broadcast_to(keep, (own, dk))
            for s in range(own):
                memory_out[b, s, h] = kept[s:s + 1, :] * mem_v[b, s, h] + ak_t[:, s:s + 1] * value[s:s + 1, :]
        loads["mix", b].wait()
        for c in copies + relayed[b]:
            c.wait_recv()
        if fast:
            every = jnp.concatenate([gated_v[b, t].reshape(n * own, width) for t in range(m)], axis=1)
        if fast:
            mixed = jnp.dot(every, mixcol_v[b].reshape(m * width, cols), preferred_element_type=F32)
            if b == 0:
                own_cols = xf_v[:, pl.ds(pl.multiple_of(tp * cols, cols), cols)]
            else:
                own_cols = xcol_v[b - 1, tp].astype(F32)
            xcol_v[b, tp] = (own_cols + mixed).astype(BF16)
            ref = xcol_v.at[b, tp]
            copies = [send(ref, ref, xs_sem.at[b, o - 1], xr_sem.at[b, o - 1], at(0, o)) for o in range(1, m)]
            arriving = copies
            if b == last:
                for c in copies:
                    c.wait_recv()
                for j in range(m):
                    x_out[:, j * cols:(j + 1) * cols] = xcol_v[b, j]
        else:
            every = gated_v[b, 0].reshape(n * own, width)
            mixed = jnp.dot(every, mix_v[b], preferred_element_type=F32)
            for j in range(m):
                piece = mixed[j * rows:(j + 1) * rows, :]
                mix_send[b, j] = piece.astype(BF16)
                mix_own[j] = piece
                xrow_v[j] = xf_v[j * rows:(j + 1) * rows, :].astype(BF16)
            copies = [
                send(mix_send.at[b, lax.rem(tp + o, m)], mix_recv.at[b, o - 1],
                     ms_sem.at[b, o - 1], mr_sem.at[b, o - 1], at(0, o))
                for o in range(1, m)
            ]
            total = mix_own[tp]
            for o, c in enumerate(copies):
                c.wait_recv()
                total = total + mix_recv[b, o].astype(F32)
            xcol_v[b, tp] = (xrow_v[tp].astype(F32) + total).astype(BF16)
            ref = xcol_v.at[b, tp]
            copies = [send(ref, ref, xs_sem.at[b, o - 1], xr_sem.at[b, o - 1], at(0, o)) for o in range(1, m)]
            for c in copies:
                c.wait_recv()
            for j in range(m):
                xf_v[j * rows:(j + 1) * rows, :] = xcol_v[b, j].astype(F32)
            if b == last:
                x_out[...] = xf_v[...].astype(BF16)
    for c in sent:
        c.wait_send()


def store_kernel(*refs):
    count = (len(refs) - 1) // 2
    sources, results, sem = refs[:count], refs[count:2 * count], refs[-1]
    copies = [pltpu.make_async_copy(a, z, sem.at[k]) for k, (a, z) in enumerate(zip(sources, results))]
    for c in copies:
        c.start()
    for c in copies:
        c.wait()


def shards(sizes, tokens, norm_gain, w_query, w_key, w_value, w_outgate, gate_weight, forget_bias, w_mix, memory, normalizer, stabilizer):
    groups, n, m = sizes
    seqs, feats = tokens.shape
    blocks, own, heads, dk, _ = memory.shape
    width = heads * dk
    rows, cols = seqs // m, feats // m
    wide = 4 * width + 128
    fast = cols % 128 == 0 and width % (16 * groups) == 0
    hbm = pl.BlockSpec(memory_space=pltpu.HBM)
    vmem = pl.BlockSpec(memory_space=pltpu.VMEM)
    dma = pltpu.SemaphoreType.DMA
    nd, nt, ng = max(n - 1, 1), max(m - 1, 1), max(groups - 1, 1)
    slow_rows = (1, 8, 128) if fast else (m, rows, feats)
    results = (
        ((seqs, feats), BF16),
        (memory.shape, F32),
        ((blocks, own, width), F32),
        ((blocks, heads, own), F32),
    )
    held = pl.pallas_call(
        functools.partial(step_kernel, sizes, fast),
        out_shape=tuple(pltpu.VMEM(shape, kind) for shape, kind in results),
        in_specs=[hbm] * 12,
        out_specs=(vmem,) * 4,
        scratch_shapes=[
            pltpu.VMEM(norm_gain.shape, F32),
            pltpu.VMEM((blocks, feats, 4 * width), BF16),
            pltpu.VMEM((blocks, heads, 2, 3 * dk), BF16),
            pltpu.VMEM((1, 16, 128) if fast else w_mix.shape, BF16),
            pltpu.VMEM((blocks, m, width, cols) if fast else (1, 1, 16, 128), BF16),
            pltpu.VMEM(memory.shape, F32),
            pltpu.VMEM((blocks, own, width), F32),
            pltpu.VMEM((blocks, heads, own), F32),
            pltpu.SMEM((heads, blocks), F32),
            pltpu.VMEM((seqs, feats), BF16),
            pltpu.VMEM((seqs, feats), F32),
            pltpu.VMEM((blocks, n, own, wide), BF16),
            pltpu.VMEM((n, own, wide), F32),
            pltpu.VMEM((blocks, nd, own, wide), BF16),
            pltpu.VMEM((blocks, m if fast else 1, n, own, width), BF16),
            pltpu.VMEM((blocks, m, seqs, cols) if fast else (blocks, m, rows, feats), BF16),
            pltpu.VMEM((blocks,) + slow_rows, BF16),
            pltpu.VMEM(slow_rows, F32),
            pltpu.VMEM((blocks, nt) + slow_rows[1:], BF16),
            pltpu.VMEM(slow_rows, BF16),
            dma((6 + 6 * blocks,)),
            dma((blocks, nd)), dma((blocks, nd)), dma((blocks, n * m)), dma((blocks, n * m)),
            dma((blocks, nt)), dma((blocks, nt)), dma((blocks, nt)), dma((blocks, nt)),
            dma((blocks, nt)), dma((blocks, nt)), dma((blocks, nt, ng)), dma((blocks, nt, ng)),
        ],
        compiler_params=pltpu.CompilerParams(collective_id=0, has_side_effects=True, vmem_limit_bytes=32 << 20),
    )(
        *(
            pltpu.with_memory_space_constraint(t, pltpu.HBM)
            for t in (
                tokens, norm_gain, w_query, w_key, w_value, w_outgate,
                jnp.swapaxes(gate_weight, 2, 3), w_mix, memory, normalizer.reshape(blocks, own, width),
                jnp.swapaxes(stabilizer, 1, 2), forget_bias.T,
            )
        ),
    )
    x, new_memory, norm, stab = pl.pallas_call(
        store_kernel,
        out_shape=tuple(jax.ShapeDtypeStruct(shape, kind) for shape, kind in results),
        in_specs=[vmem] * 4,
        out_specs=(pl.BlockSpec(memory_space=pl.ANY),) * 4,
        scratch_shapes=[dma((4,))],
    )(*(pltpu.with_memory_space_constraint(t, pltpu.VMEM) for t in held))
    return x, new_memory, norm.reshape(normalizer.shape), jnp.swapaxes(stab, 1, 2)


def solution(mesh):
    in_specs = (
        P("grp", "dp"),
        P(None, "dp"),
        P(None, "dp", "tp"),
        P(None, "dp", "tp"),
        P(None, "dp", "tp"),
        P(None, "dp", "tp"),
        P(None, "tp", None, None),
        P(None, "tp"),
        P(None, "tp", "dp"),
        P(None, ("grp", "dp"), "tp", None, None),
        P(None, ("grp", "dp"), "tp", None),
        P(None, ("grp", "dp"), "tp"),
    )
    out_specs = (
        P("grp", "dp"),
        P(None, ("grp", "dp"), "tp", None, None),
        P(None, ("grp", "dp"), "tp", None),
        P(None, ("grp", "dp"), "tp"),
    )
    body = functools.partial(shards, (mesh.shape["grp"], mesh.shape["dp"], mesh.shape["tp"]))
    return jax.shard_map(body, mesh=mesh, in_specs=in_specs, out_specs=out_specs, check_vma=False)
```
